512 devices in a mesh: ep: 128 (over z, x, core), tp: 4 (over y).
Axes of the slice: x: 4, y: 4, z: 16, core: 2. Of those that a mesh axis runs over, the one named last changes fastest.
Arguments:
- tokens: bfloat16 [3072, 2048], P('ep'), may hold values from -24 to 24
- carried_state: float32 [3072, 4, 128, 128], P('ep', 'tp'), may hold values from -4 to 4
- w_query: bfloat16 [2048, 512], P(None, 'tp'), may hold values from -0.125 to 0.125
- w_forget: bfloat16 [2048, 512], P(None, 'tp'), may hold values from -0.125 to 0.125
- w_value: bfloat16 [2048, 512], P(None, 'tp'), may hold values from -0.125 to 0.125
- forget_floor: float32 [4, 128], P('tp'), may hold values from 0.05 to 0.9
- head_gain: bfloat16 [4, 128], P('tp'), may hold values from 0.099609375 to 1.8984375
- w_out: bfloat16 [512, 2048], P('tp', 'ep'), may hold values from -0.25 to 0.25
- gain_mix: bfloat16 [2048], replicated, may hold values from 0.099609375 to 1.8984375
- gain_ffn: bfloat16 [2048], replicated, may hold values from 0.099609375 to 1.8984375
- gain_post: bfloat16 [2048], P('tp'), may hold values from 0.099609375 to 1.8984375
- w_branch_gate: bfloat16 [2048], replicated, may hold values from -0.125 to 0.125
- shared_gate: bfloat16 [2048, 512], P('ep', 'tp'), may hold values from -0.125 to 0.125
- shared_up: bfloat16 [2048, 512], P('ep', 'tp'), may hold values from -0.125 to 0.125
- shared_down: bfloat16 [512, 2048], P('tp', 'ep'), may hold values from -1.1048543 to 1.1048543
- routes: int32 [3072, 6], P('ep'), may hold values from 0 to 127, all different within a row; in each aligned block of 24 rows (0 to 23, 24 to 47, ...) at most 2 rows name the same one
- route_weights: float32 [3072, 6], P('ep'), may hold values from 0.2 to 1
- expert_gate: bfloat16 [128, 2048, 512], P('ep', None, 'tp'), may hold values from -0.125 to 0.125
- expert_up: bfloat16 [128, 2048, 512], P('ep', None, 'tp'), may hold values from -0.125 to 0.125
- expert_down: bfloat16 [128, 512, 2048], P('ep', 'tp'), may hold values from -1.1048543 to 1.1048543
Outputs:
- layer_out: bfloat16 [3072, 2048], P('ep', 'tp')
- new_state: float32 [3072, 4, 128, 128], P('ep', 'tp')
The draws below stay inside these ranges and needn't reach their ends.
Inputs may be any that keep to these rules, and one draw needn't show every extreme that they name: `routes`: among the 24 rows of one index of ep, no expert is named by more than 2 rows, a bound that some block reaches.
All inputs are finite; a program needn't handle non-finite values.
Results may differ from the reference program's by a relative error of at most 0.015.
Values may be sent and summed in bfloat16 or wider, within the bound.
No kernel may reach another device: no remote copies, remote signals or barrier semaphores. Data moves between devices by JAX's collectives and lax.ppermute only.
A program may use at most 64 MiB of HBM per device.

```python
import math
import jax
import jax.numpy as jnp
import numpy as np
from jax import lax

D = 2048
HEADS = 4
HEAD_DIM = 128
FE = 512
FS = 512
TOPK = 6
SEQ_DEV = 24
EXPERTS = 128
BATCH = 3072
CAP = 2
N_EP = 128
N_TP = 4


def rising_columns(key, shape, fan_in):
    base_key, jitter_key = jax.random.split(key)
    base = jnp.clip(jax.random.normal(base_key, shape, jnp.float32), -6.0, 6.0)
    columns = shape[-1]
    jitter = jax.random.uniform(jitter_key, (columns,), jnp.float32, -0.3, 0.3)
    position = jnp.arange(columns, dtype=jnp.float32) / columns
    scale = jnp.exp(jnp.log(3.0) * position + jitter)
    return base * scale * fan_in ** (-0.5)


def draw_expert_down(key, part):
    return rising_columns(jax.random.fold_in(key, 11), (EXPERTS, FE, D), FE).astype(jnp.bfloat16)


def draw_shared_down(key, part):
    return rising_columns(jax.random.fold_in(key, 12), (FS, D), FS).astype(jnp.bfloat16)


def with_spikes(values, rng, source, target, shards_of, factor):
    owner, partner = [(jnp.arange(values.shape[axis_at]) // (values.shape[axis_at] // shards_of)).reshape([-1 if axis == axis_at else 1 for axis in range(values.ndim)]) for axis_at in (source, target)]
    chosen = jax.random.permutation(rng, shards_of)[partner]
    strong = (owner == chosen) | (owner == (partner + shards_of // 2) % shards_of)
    return jnp.where(strong, factor * values, values)


def levels(key, shape, pieces, least, largest):
    def one(dim, parts):
        heights = jax.random.uniform(jax.random.fold_in(jax.random.fold_in(key, 6), dim), (parts,), jnp.float32, least / len(pieces), largest / len(pieces))
        return jnp.repeat(jnp.exp(heights), shape[dim] // parts).reshape((-1,) + (1,) * (len(shape) - dim - 1))

    loudness = one(*pieces[0])
    for cut in pieces[1:]:
        loudness = loudness * one(*cut)
    return loudness


def deal_out(stream_key, own, number, rows, count, top, most, skew):
    sequence = jax.random.permutation(stream_key, count)
    crowded, usual = shares(count, rows * top, most, skew, True), shares(count, rows * top, most, skew, False)
    places = jnp.arange(count)

    def named(lengths, offset_by):
        used = int((lengths > 0).sum())
        fixed = max(1, used // 4)
        moved = fixed + (places - fixed + offset_by * (used - fixed)) % max(1, count - fixed)
        return jnp.zeros((count,), jnp.int32).at[sequence[jnp.where(places < fixed, places, moved)]].set(jnp.asarray(lengths, jnp.int32))

    lengths = jnp.where(number % 4 == 0, named(crowded, number // 4), named(usual, number - number // 4 - 1))
    mixed = jax.random.permutation(jax.random.fold_in(own, 3), count)
    source_of, receiver = mixed[0:count // 2 * 2:2], mixed[1:count // 2 * 2:2]
    slack = jnp.minimum(lengths[source_of] - 1, most - lengths[receiver]) // 2
    slack = jnp.where((source_of == sequence[0]) | (receiver == sequence[0]) | (lengths[receiver] == 0), 0, jnp.maximum(slack, 0))
    moved = jax.random.randint(jax.random.fold_in(own, 4), (count // 2,), 0, 1 << 20) % (slack + 1)
    lengths = lengths.at[source_of].add(-moved).at[receiver].add(moved)
    items = jnp.searchsorted(jnp.cumsum(lengths), jnp.arange(rows * top), side="right").astype(jnp.int32)
    table = items.reshape(top, rows).T
    table = table[jax.random.permutation(jax.random.fold_in(own, 1), rows)]
    offset_by = jax.random.randint(jax.random.fold_in(own, 2), (rows, 1), 0, top)
    return jnp.take_along_axis(table, (jnp.arange(top)[None, :] + offset_by) % top, axis=1)


def shares(amount, total, limit, slope, full):
    loads = [(1 << 20) // math.isqrt(grade ** slope) + 1 for grade in range(1, amount + 1)]
    largest = limit if full else min(limit, max(-(-total // amount), total * loads[0] // sum(loads)))
    least = 1 if total - largest >= amount - 1 else 0
    counts, rest = [largest] + [least] * (amount - 1), total - largest - least * (amount - 1)
    while rest > 0:
        candidates = [i for i in range(1, amount) if counts[i] < largest] or [i for i in range(1, amount) if counts[i] < limit]
        mass, budget = sum([loads[i] for i in candidates]), rest
        for i in candidates:
            extra = min(limit - counts[i], max(1, budget * loads[i] // mass), rest)
            counts[i] = counts[i] + extra
            rest = rest - extra
    return np.array(counts)


def noise(key, extent, scale, reach, cuts=(), kind=jnp.bfloat16):
    result = scale * jax.random.normal(key, extent, jnp.float32)
    if cuts:
        result = result * levels(key, extent, cuts, -0.22, 0.18)
    return jnp.clip(result, -reach, reach).astype(kind)


def bell_draw_with(own_key, shape, spread, most, shards, heavy, kind=jnp.bfloat16):
    result = spread * jax.random.normal(own_key, shape, jnp.float32)
    if shards:
        result = result * levels(own_key, shape, shards, -0.22, 0.18)
    return jnp.clip(with_spikes(result, jax.random.fold_in(own_key, 3), *heavy), -most, most).astype(kind)


def setup_inputs(seed: int = 0) -> dict:
    key_of = jax.random.split(jax.random.key(seed), 21)
    tokens = bell_draw_with(key_of[0], (BATCH, D), 1.0, 24.0, ((0, 128),), (1, 0, 128, 5.5))
    carried_state = noise(key_of[1], (BATCH, HEADS, HEAD_DIM, HEAD_DIM), 0.5, 4.0, ((0, 128), (1, 4)), jnp.float32)
    w_query = noise(key_of[2], (D, HEADS * HEAD_DIM), D ** -0.5, 0.125, ((1, 4),))
    w_forget = noise(key_of[3], (D, HEADS * HEAD_DIM), D ** -0.5, 0.125, ((1, 4),))
    w_value = noise(key_of[4], (D, HEADS * HEAD_DIM), D ** -0.5, 0.125, ((1, 4),))
    forget_floor = jnp.clip(0.05 + 0.84999998 * jax.random.uniform(key_of[5], (HEADS, HEAD_DIM), jnp.float32) ** levels(key_of[5], (HEADS, HEAD_DIM), ((0, 4),), -0.2, 0.2), 0.05, 0.9)
    head_gain = jnp.clip(1.0 + 0.18 * jax.random.normal(key_of[6], (HEADS, HEAD_DIM), jnp.float32), 0.099609375, 1.8984375).astype(jnp.bfloat16)
    w_out = noise(key_of[7], (HEADS * HEAD_DIM, D), (HEADS * HEAD_DIM) ** -0.5, 0.25, ((0, 4), (1, 128)))
    gain_mix = jnp.clip(1.0 + 0.18 * jax.random.normal(key_of[8], (D,), jnp.float32), 0.099609375, 1.8984375).astype(jnp.bfloat16)
    gain_ffn = jnp.clip(1.0 + 0.18 * jax.random.normal(key_of[9], (D,), jnp.float32), 0.099609375, 1.8984375).astype(jnp.bfloat16)
    gain_post = jnp.clip(1.0 + 0.18 * jax.random.normal(key_of[10], (D,), jnp.float32), 0.099609375, 1.8984375).astype(jnp.bfloat16)
    w_branch_gate = noise(key_of[11], (D,), D ** -0.5, 0.125)
    shared_gate = noise(key_of[12], (D, FS), D ** -0.5, 0.125, ((0, 128), (1, 4)))
    shared_up = noise(key_of[13], (D, FS), D ** -0.5, 0.125, ((0, 128), (1, 4)))
    shared_down = draw_shared_down(jax.random.fold_in(key_of[20], 71), 0)
    routes_keys = jax.random.split(jax.random.fold_in(key_of[15], 1), BATCH // SEQ_DEV)
    routes_turns = jax.random.permutation(jax.random.fold_in(key_of[15], 3), BATCH // SEQ_DEV)
    routes = jax.vmap(lambda own, number: deal_out(jax.random.fold_in(key_of[15], 2), own, number, SEQ_DEV, EXPERTS, TOPK, CAP, 0))(routes_keys, routes_turns).reshape((BATCH, TOPK))
    route_weights = jnp.clip(0.2 + 0.8 * jax.random.uniform(key_of[16], (BATCH, TOPK), jnp.float32) ** levels(key_of[16], (BATCH, TOPK), ((0, 128),), -0.2, 0.2), 0.2, 1.0)
    expert_gate = noise(key_of[17], (EXPERTS, D, FE), D ** -0.5, 0.125, ((0, 128), (2, 4)))
    expert_up = noise(key_of[18], (EXPERTS, D, FE), D ** -0.5, 0.125, ((0, 128), (2, 4)))
    expert_down = draw_expert_down(jax.random.fold_in(key_of[20], 71), 0)
    return dict(tokens=tokens, carried_state=carried_state, w_query=w_query, w_forget=w_forget, w_value=w_value, forget_floor=forget_floor, head_gain=head_gain, w_out=w_out, gain_mix=gain_mix, gain_ffn=gain_ffn, gain_post=gain_post, w_branch_gate=w_branch_gate, shared_gate=shared_gate, shared_up=shared_up, shared_down=shared_down, routes=routes, route_weights=route_weights, expert_gate=expert_gate, expert_up=expert_up, expert_down=expert_down)


epsilon = 1e-06

def rmsnorm(values_in, gain):
    scale = lax.rsqrt(lax.optimization_barrier(jnp.mean(values_in * values_in, axis=-1, keepdims=True)) + epsilon)
    return values_in * scale * gain.astype(jnp.float32)

def group_partials(acts, weight):
    batch_rows = acts.shape[0]
    inner = acts.shape[1] // N_TP
    groups = acts.reshape(batch_rows, N_TP, inner).astype(jnp.float32)
    weight_groups = weight.reshape(N_TP, inner, weight.shape[1]).astype(jnp.float32)
    partials = jnp.einsum('btk,tkd->btd', groups, weight_groups).astype(jnp.bfloat16)
    return lax.optimization_barrier(jnp.sum(partials.astype(jnp.float32), axis=1)).astype(jnp.bfloat16)

def reference(tokens, carried_state, w_query, w_forget, w_value, forget_floor, head_gain, w_out, gain_mix, gain_ffn, gain_post, w_branch_gate, shared_gate, shared_up, shared_down, routes, route_weights, expert_gate, expert_up, expert_down):
    batch_rows = tokens.shape[0]
    normed = rmsnorm(tokens.astype(jnp.float32), gain_mix).astype(jnp.bfloat16)
    queries = jax.nn.silu(jnp.dot(normed, w_query, preferred_element_type=jnp.float32))
    forget_pre = jnp.dot(normed, w_forget, preferred_element_type=jnp.float32)
    values_in = jnp.dot(normed, w_value, preferred_element_type=jnp.float32)
    queries = queries.reshape(batch_rows, HEADS, HEAD_DIM)
    forget_pre = forget_pre.reshape(batch_rows, HEADS, HEAD_DIM)
    values_in = values_in.reshape(batch_rows, HEADS, HEAD_DIM)
    forget = forget_floor + (1.0 - forget_floor) * jax.nn.sigmoid(forget_pre)
    keys_in = (1.0 - forget_floor) * jax.nn.sigmoid(-forget_pre)
    new_state = forget[..., None] * carried_state + keys_in[..., None] * values_in[:, :, None, :]
    readout = jnp.einsum('bhd,bhdv->bhv', queries, new_state, precision=lax.Precision.HIGHEST)
    head_out = rmsnorm(readout, head_gain).astype(jnp.bfloat16).reshape(batch_rows, HEADS * HEAD_DIM)
    mixed = group_partials(head_out, w_out)
    resid = (tokens.astype(jnp.float32) + mixed.astype(jnp.float32)).astype(jnp.bfloat16)
    hnorm = rmsnorm(resid.astype(jnp.float32), gain_ffn).astype(jnp.bfloat16)
    branch_mix = jax.nn.sigmoid(jnp.dot(hnorm, w_branch_gate, preferred_element_type=jnp.float32))
    gate_pre = jnp.dot(hnorm, shared_gate, preferred_element_type=jnp.float32)
    up_pre = jnp.dot(hnorm, shared_up, preferred_element_type=jnp.float32)
    shared_hidden = (jax.nn.silu(gate_pre) * up_pre).astype(jnp.bfloat16)
    shared_out = group_partials(shared_hidden, shared_down)
    blocks = routes.reshape(N_EP, SEQ_DEV * TOPK)
    onehot = (blocks[:, :, None] == jnp.arange(EXPERTS, dtype=jnp.int32)[None, None, :]).astype(jnp.int32)
    earlier = jnp.cumsum(onehot, axis=1) - onehot
    slot_rank = lax.optimization_barrier(jnp.sum(earlier * onehot, axis=2)).reshape(-1).astype(jnp.int32)
    flat_routes = routes.reshape(-1).astype(jnp.int32)
    token_ids = (jnp.arange(batch_rows * TOPK, dtype=jnp.int32) // TOPK).astype(jnp.int32)
    source = (token_ids // SEQ_DEV).astype(jnp.int32)
    table = jnp.full((EXPERTS, N_EP, CAP), batch_rows, jnp.int32)
    table = table.at[flat_routes, source, slot_rank].set(token_ids)
    padded = jnp.concatenate([hnorm, jnp.zeros((1, D), jnp.bfloat16)], axis=0)

    def one_expert(operands):
        slots, gate_weight, up_weight, down_weight = operands
        rows_in = padded[slots.reshape(-1)]
        expert_gate_pre = jnp.dot(rows_in, gate_weight, preferred_element_type=jnp.float32)
        expert_up_pre = jnp.dot(rows_in, up_weight, preferred_element_type=jnp.float32)
        expert_hidden = (jax.nn.silu(expert_gate_pre) * expert_up_pre).astype(jnp.bfloat16)
        return group_partials(expert_hidden, down_weight)
    results = lax.map(one_expert, (table, expert_gate, expert_up, expert_down))
    picked = results.reshape(EXPERTS, N_EP, CAP, D)[flat_routes, source, slot_rank]
    picked = picked.astype(jnp.float32).reshape(batch_rows, TOPK, D)
    routed = lax.optimization_barrier(jnp.sum(picked * route_weights[:, :, None], axis=1))
    branch_sum = routed + branch_mix[:, None] * shared_out.astype(jnp.float32)
    layer_out = (resid.astype(jnp.float32) + rmsnorm(branch_sum, gain_post)).astype(jnp.bfloat16)
    return (layer_out, new_state)
```

```python
import jax
import jax.numpy as jnp
from jax import lax
from jax.experimental import pallas as pl
from jax.experimental.pallas import tpu as pltpu
from jax.sharding import Mesh
from jax.sharding import PartitionSpec as P

EP = ("ep_0", "ep_1", "ep_2")
epsilon = 1e-06
BF = jnp.bfloat16
F32 = jnp.float32
NT = (((1,), (1,)), ((), ()))


def exchanged(value, axes, name):
    with jax.named_scope(name):
        return lax.all_to_all(value, axes, 0, 0, tiled=True)


def to_all(value, axes, name):
    devices = lax.axis_size(axes)
    return exchanged(jnp.broadcast_to(value[None], (devices, *value.shape)), axes, name)


def rmsnorm(values_in, gain):
    scale = lax.rsqrt(jnp.mean(values_in * values_in, axis=-1, keepdims=True) + epsilon)
    return values_in * scale * gain.astype(F32)


def expert_body(
    x, gain, mix_w, gate_w, up_w, down_w, sgate_w, sup_w, sdown_w, out, mix, hn
):
    n_tp, total, slice_width = x.shape
    width = n_tp * slice_width
    own = mix.shape[0]
    rows = total - own
    squares = jnp.zeros((total, 1), F32)
    for j in range(n_tp):
        wide = x[j].astype(F32)
        squares = squares + jnp.sum(wide * wide, axis=1, keepdims=True)
    scale = lax.rsqrt(squares / width + epsilon)
    logits = jnp.zeros((own, 1), F32)
    for j in range(n_tp):
        cols = pl.ds(j * slice_width, slice_width)
        part = (x[j].astype(F32) * scale * gain[:, cols].astype(F32)).astype(BF)
        hn[:, cols] = part
        logits = logits + jnp.sum(
            part[rows:].astype(F32) * mix_w[:, cols].astype(F32), axis=1, keepdims=True
        )
    mix[...] = jnp.broadcast_to(jax.nn.sigmoid(logits), mix.shape)
    routed = hn[:rows, :]
    gate_pre = jnp.dot(routed, gate_w[...], preferred_element_type=F32)
    up_pre = jnp.dot(routed, up_w[...], preferred_element_type=F32)
    hidden = (gate_pre * jax.nn.sigmoid(gate_pre) * up_pre).astype(BF)
    mine = hn[rows:, :]
    gate_pre = jnp.dot(mine, sgate_w[...], preferred_element_type=F32)
    up_pre = jnp.dot(mine, sup_w[...], preferred_element_type=F32)
    shared_hidden = (gate_pre * jax.nn.sigmoid(gate_pre) * up_pre).astype(BF)
    for j in range(n_tp):
        cols = pl.ds(j * slice_width, slice_width)
        out[j, :rows, :] = jnp.dot(hidden, down_w[:, cols], preferred_element_type=F32).astype(BF)
        out[j, rows:, :] = lax.dot_general(
            shared_hidden, sdown_w[cols, :], NT, preferred_element_type=F32
        ).astype(BF)


def expert_kernel(own, x, *rest):
    n_tp, total, slice_width = x.shape
    vmem = pl.BlockSpec(memory_space=pltpu.VMEM)
    return pl.pallas_call(
        expert_body,
        out_shape=(
            jax.ShapeDtypeStruct(x.shape, BF),
            jax.ShapeDtypeStruct((own, 128), F32),
        ),
        in_specs=[vmem] * 9,
        out_specs=(vmem, vmem),
        scratch_shapes=[pltpu.VMEM((total, n_tp * slice_width), BF)],
        compiler_params=pltpu.CompilerParams(vmem_limit_bytes=32 * 1024 * 1024),
        name="expert",
    )(x, *rest)


def shards(
    tokens,
    carried_state,
    w_query,
    w_forget,
    w_value,
    forget_floor,
    head_gain,
    w_out,
    gain_mix,
    gain_ffn,
    gain_post,
    w_branch_gate,
    shared_gate,
    shared_up,
    shared_down,
    routes,
    route_weights,
    expert_gate,
    expert_up,
    expert_down,
):
    seq_rows, model_width = tokens.shape
    head_dim = carried_state.shape[2]
    n_ep = lax.axis_size(EP)
    n_tp = lax.axis_size("tp")
    slice_width = model_width // n_tp
    blocks = slice_width // 128
    here = lax.axis_index("tp")
    parts = to_all(jnp.stack([w_out.T, shared_gate, shared_up, shared_down.T]), "ep_0", "wz")
    wt = to_all(parts[:, 0], "ep_1", "wx")
    wt = to_all(wt, "ep_2", "wc")
    wt = wt.transpose(2, 1, 0, 3, 4).reshape(model_width, head_dim)
    expert_ids = lax.broadcasted_iota(jnp.int32, (1, 1, n_ep), 2)
    hits = routes[:, :, None] == expert_ids
    named = jnp.any(hits, axis=1).astype(BF)
    tri = (
        lax.broadcasted_iota(jnp.int32, (seq_rows, seq_rows), 0)
        > lax.broadcasted_iota(jnp.int32, (seq_rows, seq_rows), 1)
    ).astype(BF)
    rank = jnp.dot(tri, named, preferred_element_type=F32)
    slots = [
        jnp.where((named > 0) & (rank == s), 1.0, 0.0).astype(BF) for s in range(2)
    ]
    slot = jnp.stack(slots, axis=2)
    weights = jnp.sum(jnp.where(hits, route_weights[:, :, None], 0.0), axis=1)
    normed = rmsnorm(tokens.astype(F32), gain_mix).astype(BF)
    queries = jax.nn.silu(jnp.dot(normed, w_query, preferred_element_type=F32))
    forget_pre = jnp.dot(normed, w_forget, preferred_element_type=F32)
    values_in = jnp.dot(normed, w_value, preferred_element_type=F32)
    queries = queries.reshape(seq_rows, 1, head_dim)
    forget_pre = forget_pre.reshape(seq_rows, 1, head_dim)
    values_in = values_in.reshape(seq_rows, 1, head_dim)
    forget = forget_floor + (1.0 - forget_floor) * jax.nn.sigmoid(forget_pre)
    keys_in = (1.0 - forget_floor) * jax.nn.sigmoid(-forget_pre)
    new_state = forget[..., None] * carried_state + keys_in[..., None] * values_in[:, :, None, :]
    readout = jnp.einsum("bhd,bhdv->bhv", queries, new_state, precision=lax.Precision.HIGHEST)
    head_out = rmsnorm(readout, head_gain).astype(BF).reshape(seq_rows, head_dim)
    terms = lax.dot_general(head_out, wt, NT, preferred_element_type=F32).astype(BF)
    terms = terms.reshape(seq_rows, n_tp, slice_width).transpose(1, 0, 2)
    mixed = jnp.sum(exchanged(terms, "tp", "mix").astype(F32), axis=0).astype(BF)
    token_slice = lax.dynamic_slice_in_dim(tokens, here * slice_width, slice_width, 1)
    resid = (token_slice.astype(F32) + mixed.astype(F32)).astype(BF)
    sent = jnp.einsum("bes,bd->esd", slot, resid, preferred_element_type=F32).astype(BF)
    arrived = exchanged(sent.reshape(n_ep, 2 * blocks, 128), EP, "disp")
    arrived = arrived.reshape(2 * n_ep, slice_width)
    with jax.named_scope("sx"):
        shared = lax.all_gather(parts[:, 1:], "ep_1")
    with jax.named_scope("sc"):
        other = lax.ppermute(shared, "ep_2", [(0, 1), (1, 0)])
        first = lax.axis_index("ep_2") == 0
        shared = jnp.stack([jnp.where(first, shared, other), jnp.where(first, other, shared)])
    shared = shared.transpose(3, 2, 1, 0, 4, 5).reshape(3, model_width, head_dim)
    x = to_all(jnp.concatenate([arrived, resid], axis=0), "tp", "rows")
    down_terms, mix = expert_kernel(
        seq_rows,
        x,
        gain_ffn[None],
        w_branch_gate[None],
        expert_gate[0],
        expert_up[0],
        expert_down[0],
        shared[0],
        shared[1],
        shared[2],
    )
    summed = jnp.sum(exchanged(down_terms, "tp", "rs").astype(F32), axis=0).astype(BF)
    returned = exchanged(summed[: 2 * n_ep].reshape(n_ep, 2 * blocks, 128), EP, "ret")
    shared_out = summed[2 * n_ep :]
    combine = weights[:, :, None] * slot.astype(F32)
    routed = jnp.dot(
        combine.reshape(seq_rows, 2 * n_ep),
        returned.reshape(2 * n_ep, slice_width).astype(F32),
        precision=lax.Precision.HIGHEST,
    )
    branch_sum = routed + mix[:, :1] * shared_out.astype(F32)
    square_part = jnp.sum(branch_sum * branch_sum, axis=1)
    square_total = jnp.sum(to_all(square_part, "tp", "sq"), axis=0)
    norm_scale = lax.rsqrt(square_total / model_width + epsilon)
    layer_out = resid.astype(F32) + branch_sum * norm_scale[:, None] * gain_post.astype(F32)
    return (layer_out.astype(BF), new_state)


def solution(mesh):
    torus = Mesh(mesh.devices.reshape(16, 4, 2, mesh.shape["tp"]), ("ep_0", "ep_1", "ep_2", "tp"))
    in_specs = (
        P(EP, None),
        P(EP, "tp", None, None),
        P(None, "tp"),
        P(None, "tp"),
        P(None, "tp"),
        P("tp", None),
        P("tp", None),
        P("tp", EP),
        P(),
        P(),
        P("tp"),
        P(),
        P(EP, "tp"),
        P(EP, "tp"),
        P("tp", EP),
        P(EP, None),
        P(EP, None),
        P(EP, None, "tp"),
        P(EP, None, "tp"),
        P(EP, "tp", None),
    )
    out_specs = (P(EP, "tp"), P(EP, "tp", None, None))
    return jax.shard_map(
        shards, mesh=torus, in_specs=in_specs, out_specs=out_specs, check_vma=False
    )
```

```python
import jax
import jax.numpy as jnp
from jax import lax
from jax.experimental import pallas as pl
from jax.experimental.pallas import tpu as pltpu
from jax.sharding import Mesh
from jax.sharding import PartitionSpec as P

EP = ("ep_0", "ep_1", "ep_2")
epsilon = 1e-06
BF = jnp.bfloat16
F32 = jnp.float32
NT = (((1,), (1,)), ((), ()))


def exchanged(value, axes):
    return lax.all_to_all(value, axes, 0, 0, tiled=True)


def to_all(value, axes):
    devices = lax.axis_size(axes)
    return exchanged(jnp.broadcast_to(value[None], (devices, *value.shape)), axes)


def rmsnorm(values_in, gain):
    scale = lax.rsqrt(jnp.mean(values_in * values_in, axis=-1, keepdims=True) + epsilon)
    return values_in * scale * gain.astype(F32)


def from_z_order(cores, zs, inverse):
    n = cores * zs * 2
    core_major = lax.broadcasted_iota(jnp.int32, (n, n), 1 if inverse else 0)
    z_major = lax.broadcasted_iota(jnp.int32, (n, n), 0 if inverse else 1)
    core, z, slot = core_major // (2 * zs), (core_major // 2) % zs, core_major % 2
    return jnp.where(z_major == (z * cores + core) * 2 + slot, 1.0, 0.0).astype(BF)


def vmem_call(body, out_shape, args, scratch=(), limit=32):
    vmem = pl.BlockSpec(memory_space=pltpu.VMEM)
    return pl.pallas_call(
        body,
        out_shape=out_shape,
        in_specs=[vmem] * len(args),
        out_specs=jax.tree.map(lambda _: vmem, out_shape),
        scratch_shapes=list(scratch),
        compiler_params=pltpu.CompilerParams(vmem_limit_bytes=limit * 1024 * 1024),
    )(*args)


def dispatch_body(terms, places, tok, chosen, resid, send):
    mixed = jnp.zeros(tok.shape, F32)
    for k in range(terms.shape[0]):
        part = terms[k, 0].astype(F32)
        for t in range(1, terms.shape[1]):
            part = part + terms[k, t].astype(F32)
        mixed = mixed + jnp.dot(part.astype(BF), places[k], preferred_element_type=F32)
    summed = (tok[...].astype(F32) + mixed).astype(BF)
    resid[...] = summed
    send[...] = jnp.dot(chosen[...], summed, preferred_element_type=F32).astype(BF)


def spread_body(arrived, out):
    cores, n_tp, rows, width = out.shape
    perm = from_z_order(cores, rows // 2, False)
    moved = jnp.dot(perm, arrived[...], preferred_element_type=F32).astype(BF)
    for t in range(n_tp):
        out[:, t] = moved.reshape(cores, rows, width)


def collect_body(terms, out):
    cores, n_tp, rows, width = terms.shape
    total = terms[:, 0].astype(F32)
    for t in range(1, n_tp):
        total = total + terms[:, t].astype(F32)
    perm = from_z_order(cores, rows // 2, True)
    total = total.astype(BF).reshape(cores * rows, width)
    out[...] = jnp.dot(perm, total, preferred_element_type=F32).astype(BF)


def normed_columns(x, gain, hn):
    slice_width = hn.shape[1] // x[0]
    squares = None
    for j in range(x[0]):
        wide = x[1](j).astype(F32)
        part = jnp.sum(wide * wide, axis=1, keepdims=True)
        squares = part if squares is None else squares + part
    scale = lax.rsqrt(squares / hn.shape[1] + epsilon)
    for j in range(x[0]):
        cols = pl.ds(j * slice_width, slice_width)
        hn[:, cols] = (x[1](j).astype(F32) * scale * gain[:, cols].astype(F32)).astype(BF)


def expert_body(x, gain, gate_hbm, up_hbm, down_hbm, out, hn, gate_w, up_w, down_w, sems):
    cores, n_tp, rows, slice_width = x.shape
    total = cores * rows
    copies = [
        pltpu.make_async_copy(src, dst, sems.at[k])
        for k, (src, dst) in enumerate(
            ((gate_hbm, gate_w), (up_hbm, up_w), (down_hbm, down_w))
        )
    ]
    for copy in copies:
        copy.start()
    normed_columns((n_tp, lambda j: x[:, j].reshape(total, slice_width)), gain, hn)
    copies[0].wait()
    gate_pre = jnp.dot(hn[...], gate_w[...], preferred_element_type=F32)
    copies[1].wait()
    up_pre = jnp.dot(hn[...], up_w[...], preferred_element_type=F32)
    hidden = (gate_pre * jax.nn.sigmoid(gate_pre) * up_pre).astype(BF)
    copies[2].wait()
    for j in range(n_tp):
        cols = pl.ds(j * slice_width, slice_width)
        part = jnp.dot(hidden, down_w[:, cols], preferred_element_type=F32).astype(BF)
        out[:, j] = part.reshape(cores, rows, slice_width)


def expert_kernel(x, gain, gate_w, up_w, down_w):
    cores, n_tp, rows, slice_width = x.shape
    vmem = pl.BlockSpec(memory_space=pltpu.VMEM)
    hbm = pl.BlockSpec(memory_space=pl.ANY)
    return pl.pallas_call(
        expert_body,
        out_shape=jax.ShapeDtypeStruct(x.shape, BF),
        in_specs=[vmem, vmem, hbm, hbm, hbm],
        out_specs=vmem,
        scratch_shapes=[
            pltpu.VMEM((cores * rows, n_tp * slice_width), BF),
            pltpu.VMEM(gate_w.shape, BF),
            pltpu.VMEM(up_w.shape, BF),
            pltpu.VMEM(down_w.shape, BF),
            pltpu.SemaphoreType.DMA((3,)),
        ],
        compiler_params=pltpu.CompilerParams(vmem_limit_bytes=32 * 1024 * 1024),
        name="expert",
    )(x, gain, gate_w, up_w, down_w)


def shared_body(x, gain, mix_w, gate_w, up_w, down_w, out, mix, hn):
    n_tp = x.shape[0]
    normed_columns((n_tp, lambda j: x[j]), gain, hn)
    logits = jnp.sum(hn[...].astype(F32) * mix_w[...].astype(F32), axis=1, keepdims=True)
    mix[...] = jnp.broadcast_to(jax.nn.sigmoid(logits), mix.shape)
    gate_pre = jnp.dot(hn[...], gate_w[...], preferred_element_type=F32)
    up_pre = jnp.dot(hn[...], up_w[...], preferred_element_type=F32)
    hidden = (gate_pre * jax.nn.sigmoid(gate_pre) * up_pre).astype(BF)
    out[...] = lax.dot_general(hidden, down_w[...], NT, preferred_element_type=F32).astype(BF)


def shards(
    tokens,
    carried_state,
    w_query,
    w_forget,
    w_value,
    forget_floor,
    head_gain,
    w_out,
    gain_mix,
    gain_ffn,
    gain_post,
    w_branch_gate,
    shared_gate,
    shared_up,
    shared_down,
    routes,
    route_weights,
    expert_gate,
    expert_up,
    expert_down,
):
    seq_rows, model_width = tokens.shape
    head_dim = carried_state.shape[2]
    n_ep = lax.axis_size(EP)
    n_z = lax.axis_size("ep_0")
    n_tp = lax.axis_size("tp")
    cores = n_ep // n_z
    piece = w_out.shape[1]
    slice_width = model_width // n_tp
    slots_all = 2 * n_ep
    here = lax.axis_index("tp")
    parts = to_all(jnp.stack([w_out.T, shared_gate, shared_up, shared_down.T]), "ep_0")
    column = lax.broadcasted_iota(jnp.int32, (1, 1, slots_all), 2)
    hits = routes[:, :, None] == column // 2
    named = jnp.any(hits, axis=1).astype(BF)
    tri = (
        lax.broadcasted_iota(jnp.int32, (seq_rows, seq_rows), 0)
        > lax.broadcasted_iota(jnp.int32, (seq_rows, seq_rows), 1)
    ).astype(BF)
    rank = jnp.dot(tri, named, preferred_element_type=F32)
    taken = (named > 0) & (rank == (column[0] % 2).astype(F32))
    chosen = jnp.where(taken, 1.0, 0.0).astype(BF).T
    combine = jnp.where(taken, jnp.sum(jnp.where(hits, route_weights[:, :, None], 0.0), axis=1), 0.0)
    normed = rmsnorm(tokens.astype(F32), gain_mix).astype(BF)
    queries = jax.nn.silu(jnp.dot(normed, w_query, preferred_element_type=F32))
    forget_pre = jnp.dot(normed, w_forget, preferred_element_type=F32)
    values_in = jnp.dot(normed, w_value, preferred_element_type=F32)
    queries = queries.reshape(seq_rows, 1, head_dim)
    forget_pre = forget_pre.reshape(seq_rows, 1, head_dim)
    values_in = values_in.reshape(seq_rows, 1, head_dim)
    forget = forget_floor + (1.0 - forget_floor) * jax.nn.sigmoid(forget_pre)
    keys_in = (1.0 - forget_floor) * jax.nn.sigmoid(-forget_pre)
    new_state = forget[..., None] * carried_state + keys_in[..., None] * values_in[:, :, None, :]
    readout = jnp.einsum("bhd,bhdv->bhv", queries, new_state, precision=lax.Precision.HIGHEST)
    head_out = rmsnorm(readout, head_gain).astype(BF).reshape(seq_rows, head_dim)
    heads = lax.all_gather(head_out, "ep_2")
    heads = lax.all_gather(heads, "ep_1").reshape(cores * seq_rows, head_dim)
    line_w = parts[:, 0].reshape(n_z * piece, head_dim)
    terms = lax.dot_general(heads, line_w, NT, preferred_element_type=F32).astype(BF)
    own = n_z * piece // n_tp
    per = 128 // own
    terms = terms.reshape(cores, 1, seq_rows, n_tp // per, 128)
    terms = jnp.broadcast_to(terms, (cores, per, seq_rows, n_tp // per, 128))
    terms = terms.transpose(0, 3, 1, 2, 4).reshape(cores * n_tp, seq_rows, 128)
    terms = exchanged(terms, ("ep_1", "ep_2", "tp"))
    terms = terms.reshape(cores, n_tp, seq_rows, 128)
    core = lax.broadcasted_iota(jnp.int32, (cores, 128, slice_width), 0)
    lane = lax.broadcasted_iota(jnp.int32, (cores, 128, slice_width), 1) - own * (here % per)
    target = lax.broadcasted_iota(jnp.int32, (cores, 128, slice_width), 2)
    places = (
        (lane >= 0)
        & (lane < own)
        & (target == (lane // piece * cores + core) * piece + lane % piece)
    )
    places = jnp.where(places, 1.0, 0.0).astype(BF)
    token_slice = lax.dynamic_slice_in_dim(tokens, here * slice_width, slice_width, 1)
    resid, send = vmem_call(
        dispatch_body,
        (
            jax.ShapeDtypeStruct((seq_rows, slice_width), BF),
            jax.ShapeDtypeStruct((slots_all, slice_width), BF),
        ),
        (terms, places, token_slice, chosen),
    )
    arrived = exchanged(send.reshape(n_z, 2 * cores, slice_width), "ep_0")
    mine = lax.all_gather(resid, "tp")
    spread = vmem_call(
        spread_body,
        jax.ShapeDtypeStruct((cores, n_tp, 2 * n_z, slice_width), BF),
        (arrived.reshape(slots_all, slice_width),),
    )
    plane = (cores * n_tp, 2 * n_z, slice_width)
    x = exchanged(spread.reshape(plane), ("ep_1", "ep_2", "tp")).reshape(spread.shape)
    down_terms = expert_kernel(x, gain_ffn[None], expert_gate[0], expert_up[0], expert_down[0])
    down_terms = exchanged(down_terms.reshape(plane), ("ep_1", "ep_2", "tp"))
    summed = vmem_call(
        collect_body,
        jax.ShapeDtypeStruct((slots_all, slice_width), BF),
        (down_terms.reshape(spread.shape),),
    )
    returned = exchanged(summed.reshape(n_z, 2 * cores, slice_width), "ep_0")
    returned = returned.reshape(slots_all, slice_width)
    shared = lax.all_gather(parts[:, 1:], "ep_1")
    other = lax.ppermute(shared, "ep_2", [(0, 1), (1, 0)])
    first = lax.axis_index("ep_2") == 0
    shared = jnp.stack([jnp.where(first, shared, other), jnp.where(first, other, shared)])
    shared = shared.transpose(3, 2, 1, 0, 4, 5).reshape(3, model_width, head_dim)
    shared_terms, mix = vmem_call(
        shared_body,
        (
            jax.ShapeDtypeStruct((seq_rows, model_width), BF),
            jax.ShapeDtypeStruct((seq_rows, 128), F32),
        ),
        (mine, gain_ffn[None], w_branch_gate[None], shared[0], shared[1], shared[2]),
        (pltpu.VMEM((seq_rows, model_width), BF),),
    )
    shared_terms = lax.all_gather(shared_terms, "tp")
    shared_terms = lax.dynamic_slice_in_dim(shared_terms, here * slice_width, slice_width, 2)
    shared_out = jnp.sum(shared_terms.astype(F32), axis=0).astype(BF)
    routed = jnp.dot(combine, returned.astype(F32), precision=lax.Precision.HIGHEST)
    branch_sum = routed + mix[:, :1] * shared_out.astype(F32)
    square_part = jnp.sum(branch_sum * branch_sum, axis=1)
    square_total = jnp.sum(to_all(square_part, "tp"), axis=0)
    norm_scale = lax.rsqrt(square_total / model_width + epsilon)
    layer_out = resid.astype(F32) + branch_sum * norm_scale[:, None] * gain_post.astype(F32)
    return (layer_out.astype(BF), new_state)


def solution(mesh):
    torus = Mesh(mesh.devices.reshape(16, 4, 2, mesh.shape["tp"]), ("ep_0", "ep_1", "ep_2", "tp"))
    in_specs = (
        P(EP, None),
        P(EP, "tp", None, None),
        P(None, "tp"),
        P(None, "tp"),
        P(None, "tp"),
        P("tp", None),
        P("tp", None),
        P("tp", EP),
        P(),
        P(),
        P("tp"),
        P(),
        P(EP, "tp"),
        P(EP, "tp"),
        P("tp", EP),
        P(EP, None),
        P(EP, None),
        P(EP, None, "tp"),
        P(EP, None, "tp"),
        P(EP, "tp", None),
    )
    out_specs = (P(EP, "tp"), P(EP, "tp", None, None))

    return jax.shard_map(
        shards, mesh=torus, in_specs=in_specs, out_specs=out_specs, check_vma=False
    )
```

```python
import functools

import jax
import jax.numpy as jnp
from jax import lax
from jax.experimental import pallas as pl
from jax.experimental.pallas import tpu as pltpu
from jax.sharding import Mesh
from jax.sharding import PartitionSpec as P

EP = ("ep_0", "ep_1", "ep_2")
epsilon = 1e-06
BF = jnp.bfloat16
F32 = jnp.float32
NT = (((1,), (1,)), ((), ()))


def exchanged(value, axes):
    return lax.all_to_all(value, axes, 0, 0, tiled=True)


def to_all(value, axes):
    devices = lax.axis_size(axes)
    return exchanged(jnp.broadcast_to(value[None], (devices, *value.shape)), axes)


def from_z_order(cores, zs, inverse):
    n = cores * zs * 2
    core_major = lax.broadcasted_iota(jnp.int32, (n, n), 1 if inverse else 0)
    z_major = lax.broadcasted_iota(jnp.int32, (n, n), 0 if inverse else 1)
    core, z, slot = core_major // (2 * zs), (core_major // 2) % zs, core_major % 2
    return jnp.where(z_major == (z * cores + core) * 2 + slot, 1.0, 0.0).astype(BF)


def vmem_call(body, out_shape, args, scratch=(), limit=32):
    vmem = pl.BlockSpec(memory_space=pltpu.VMEM)
    return pl.pallas_call(
        body,
        out_shape=out_shape,
        in_specs=[vmem] * len(args),
        out_specs=jax.tree.map(lambda _: vmem, out_shape),
        scratch_shapes=list(scratch),
        compiler_params=pltpu.CompilerParams(vmem_limit_bytes=limit * 1024 * 1024),
    )(*args)


def recurrence_body(
    tokens, gain, w_query, w_forget, w_value, floor, head_gain, state, new_hbm, out, new, read, sem
):
    rows = tokens.shape[0]
    wide = tokens[...].astype(F32)
    scale = lax.rsqrt(jnp.mean(wide * wide, axis=1, keepdims=True) + epsilon)
    normed = (wide * scale * gain[...].astype(F32)).astype(BF)
    query = jnp.dot(normed, w_query[...], preferred_element_type=F32)
    query = (query * jax.nn.sigmoid(query)).T
    pre = jnp.dot(normed, w_forget[...], preferred_element_type=F32)
    values = jnp.dot(normed, w_value[...], preferred_element_type=F32)
    low = floor[...]
    forget = (low + (1.0 - low) * jax.nn.sigmoid(pre)).T
    keys = ((1.0 - low) * jax.nn.sigmoid(-pre)).T
    half = rows // 2
    copies = [
        pltpu.make_async_copy(new.at[pl.ds(k * half, half)], new_hbm.at[pl.ds(k * half, half)], sem.at[k])
        for k in range(2)
    ]
    for b in range(rows):
        fresh = forget[:, b : b + 1] * state[b] + keys[:, b : b + 1] * values[b : b + 1, :]
        new[b] = fresh
        read[b : b + 1, :] = jnp.sum(query[:, b : b + 1] * fresh, axis=0, keepdims=True)
        if (b + 1) % half == 0:
            copies[b // half].start()
    readout = read[...]
    scale = lax.rsqrt(jnp.mean(readout * readout, axis=1, keepdims=True) + epsilon)
    out[...] = (readout * scale * head_gain[...].astype(F32)).astype(BF)
    for copy in copies:
        copy.wait()


def recurrence_kernel(*args):
    tokens, state = args[0], args[-1]
    vmem = pl.BlockSpec(memory_space=pltpu.VMEM)
    hbm = pl.BlockSpec(memory_space=pl.ANY)
    return pl.pallas_call(
        recurrence_body,
        out_shape=(
            jax.ShapeDtypeStruct(state.shape, F32),
            jax.ShapeDtypeStruct((tokens.shape[0], state.shape[2]), BF),
        ),
        in_specs=[vmem] * len(args),
        out_specs=(hbm, vmem),
        scratch_shapes=[
            pltpu.VMEM(state.shape, F32),
            pltpu.VMEM((tokens.shape[0], state.shape[2]), F32),
            pltpu.SemaphoreType.DMA((2,)),
        ],
        compiler_params=pltpu.CompilerParams(vmem_limit_bytes=16 * 1024 * 1024),
        name="recurrence",
    )(*args)


def project_body(heads, parts, out):
    cores, n_tp, rows, lanes = out.shape
    n_z = parts.shape[0]
    near = n_z // n_tp
    acts = heads[...].reshape(cores * rows, heads.shape[2])
    for t in range(n_tp):
        start = t * near
        other = (t ^ 1) * near
        order = list(range(start, start + near)) + list(range(other, other + near))
        columns = jnp.concatenate([parts[z, 0] for z in order], axis=0)
        term = lax.dot_general(acts, columns, NT, preferred_element_type=F32).astype(BF)
        out[:, t] = term.reshape(cores, rows, lanes)


def dispatch_body(terms, tok, chosen, resid, send, *, piece):
    cores, n_tp, rows, lanes = terms.shape
    parts = []
    for k in range(cores):
        part = terms[k, 0].astype(F32)
        for t in range(1, n_tp):
            part = part + terms[k, t].astype(F32)
        parts.append(part.astype(BF).astype(F32))
    owner = lax.broadcasted_iota(jnp.int32, (rows, lanes), 1) // piece
    for z in range(tok.shape[1] // lanes):
        mixed = jnp.zeros((rows, lanes), F32)
        for k in range(cores):
            turn = (k - z) * piece % lanes
            moved = pltpu.roll(parts[k], turn, 1) if turn else parts[k]
            mixed = jnp.where(owner == k, moved, mixed)
        cols = pl.ds(z * lanes, lanes)
        resid[:, cols] = (tok[:, cols].astype(F32) + mixed).astype(BF)
    send[...] = jnp.dot(chosen[...], resid[...], preferred_element_type=F32).astype(BF)


def spread_body(arrived, out):
    cores, n_tp, rows, width = out.shape
    perm = from_z_order(cores, rows // 2, False)
    moved = jnp.dot(perm, arrived[...], preferred_element_type=F32).astype(BF)
    for t in range(n_tp):
        out[:, t] = moved.reshape(cores, rows, width)


def collect_body(terms, out):
    cores, n_tp, rows, width = terms.shape
    total = terms[:, 0].astype(F32)
    for t in range(1, n_tp):
        total = total + terms[:, t].astype(F32)
    perm = from_z_order(cores, rows // 2, True)
    total = total.astype(BF).reshape(cores * rows, width)
    out[...] = jnp.dot(perm, total, preferred_element_type=F32).astype(BF)


def normed_columns(x, gain, hn):
    slice_width = hn.shape[1] // x[0]
    squares = None
    for j in range(x[0]):
        wide = x[1](j).astype(F32)
        part = jnp.sum(wide * wide, axis=1, keepdims=True)
        squares = part if squares is None else squares + part
    scale = lax.rsqrt(squares / hn.shape[1] + epsilon)
    for j in range(x[0]):
        cols = pl.ds(j * slice_width, slice_width)
        hn[:, cols] = (x[1](j).astype(F32) * scale * gain[:, cols].astype(F32)).astype(BF)


def expert_body(x, gain, gate_hbm, up_hbm, down_hbm, out, hn, gate_w, up_w, down_w, sems):
    cores, n_tp, rows, slice_width = x.shape
    total = cores * rows
    copies = [
        pltpu.make_async_copy(src, dst, sems.at[k])
        for k, (src, dst) in enumerate(
            ((gate_hbm, gate_w), (up_hbm, up_w), (down_hbm, down_w))
        )
    ]
    for copy in copies:
        copy.start()
    normed_columns((n_tp, lambda j: x[:, j].reshape(total, slice_width)), gain, hn)
    copies[0].wait()
    gate_pre = jnp.dot(hn[...], gate_w[...], preferred_element_type=F32)
    copies[1].wait()
    up_pre = jnp.dot(hn[...], up_w[...], preferred_element_type=F32)
    hidden = (gate_pre * jax.nn.sigmoid(gate_pre) * up_pre).astype(BF)
    copies[2].wait()
    for j in range(n_tp):
        cols = pl.ds(j * slice_width, slice_width)
        part = jnp.dot(hidden, down_w[:, cols], preferred_element_type=F32).astype(BF)
        out[:, j] = part.reshape(cores, rows, slice_width)


def expert_kernel(x, gain, gate_w, up_w, down_w):
    cores, n_tp, rows, slice_width = x.shape
    vmem = pl.BlockSpec(memory_space=pltpu.VMEM)
    hbm = pl.BlockSpec(memory_space=pl.ANY)
    return pl.pallas_call(
        expert_body,
        out_shape=jax.ShapeDtypeStruct(x.shape, BF),
        in_specs=[vmem, vmem, hbm, hbm, hbm],
        out_specs=vmem,
        scratch_shapes=[
            pltpu.VMEM((cores * rows, n_tp * slice_width), BF),
            pltpu.VMEM(gate_w.shape, BF),
            pltpu.VMEM(up_w.shape, BF),
            pltpu.VMEM(down_w.shape, BF),
            pltpu.SemaphoreType.DMA((3,)),
        ],
        compiler_params=pltpu.CompilerParams(vmem_limit_bytes=32 * 1024 * 1024),
        name="expert",
    )(x, gain, gate_w, up_w, down_w)


def shared_body(x, gain, mix_w, gate_w, up_w, down_w, out, mix, hn):
    n_tp = x.shape[0]
    normed_columns((n_tp, lambda j: x[j]), gain, hn)
    logits = jnp.sum(hn[...].astype(F32) * mix_w[...].astype(F32), axis=1, keepdims=True)
    mix[...] = jnp.broadcast_to(jax.nn.sigmoid(logits), mix.shape)
    gate_pre = jnp.dot(hn[...], gate_w[...], preferred_element_type=F32)
    up_pre = jnp.dot(hn[...], up_w[...], preferred_element_type=F32)
    hidden = (gate_pre * jax.nn.sigmoid(gate_pre) * up_pre).astype(BF)
    out[...] = lax.dot_general(hidden, down_w[...], NT, preferred_element_type=F32).astype(BF)


def shards(
    tokens,
    carried_state,
    w_query,
    w_forget,
    w_value,
    forget_floor,
    head_gain,
    w_out,
    gain_mix,
    gain_ffn,
    gain_post,
    w_branch_gate,
    shared_gate,
    shared_up,
    shared_down,
    routes,
    route_weights,
    expert_gate,
    expert_up,
    expert_down,
):
    seq_rows, model_width = tokens.shape
    head_dim = carried_state.shape[2]
    n_ep = lax.axis_size(EP)
    n_z = lax.axis_size("ep_0")
    n_tp = lax.axis_size("tp")
    cores = n_ep // n_z
    piece = w_out.shape[1]
    slice_width = model_width // n_tp
    slots_all = 2 * n_ep
    here = lax.axis_index("tp")
    parts = to_all(jnp.stack([w_out.T, shared_gate, shared_up, shared_down.T]), "ep_0")
    column = lax.broadcasted_iota(jnp.int32, (1, 1, slots_all), 2)
    hits = routes[:, :, None] == column // 2
    named = jnp.any(hits, axis=1).astype(BF)
    tri = (
        lax.broadcasted_iota(jnp.int32, (seq_rows, seq_rows), 0)
        > lax.broadcasted_iota(jnp.int32, (seq_rows, seq_rows), 1)
    ).astype(BF)
    rank = jnp.dot(tri, named, preferred_element_type=F32)
    taken = (named > 0) & (rank == (column[0] % 2).astype(F32))
    chosen = jnp.where(taken, 1.0, 0.0).astype(BF).T
    combine = jnp.where(taken, jnp.sum(jnp.where(hits, route_weights[:, :, None], 0.0), axis=1), 0.0)
    new_state, head_out = recurrence_kernel(
        tokens,
        gain_mix[None],
        w_query,
        w_forget,
        w_value,
        forget_floor,
        head_gain,
        carried_state.reshape(seq_rows, head_dim, head_dim),
    )
    new_state = new_state.reshape(carried_state.shape)
    heads = lax.all_gather(head_out, "ep_2")
    heads = lax.all_gather(heads, "ep_1").reshape(cores, seq_rows, head_dim)
    terms = vmem_call(
        project_body, jax.ShapeDtypeStruct((cores, n_tp, seq_rows, 128), BF), (heads, parts)
    )
    terms = exchanged(
        terms.reshape(cores * n_tp, seq_rows, 128), ("ep_1", "ep_2", "tp")
    ).reshape(terms.shape)
    token_slice = lax.dynamic_slice_in_dim(tokens, here * slice_width, slice_width, 1)
    resid, send = vmem_call(
        functools.partial(dispatch_body, piece=piece),
        (
            jax.ShapeDtypeStruct((seq_rows, slice_width), BF),
            jax.ShapeDtypeStruct((slots_all, slice_width), BF),
        ),
        (terms, token_slice, chosen),
    )
    arrived = exchanged(send.reshape(n_z, 2 * cores, slice_width), "ep_0")
    mine = lax.all_gather(resid, "tp")
    spread = vmem_call(
        spread_body,
        jax.ShapeDtypeStruct((cores, n_tp, 2 * n_z, slice_width), BF),
        (arrived.reshape(slots_all, slice_width),),
    )
    plane = (cores * n_tp, 2 * n_z, slice_width)
    x = exchanged(spread.reshape(plane), ("ep_1", "ep_2", "tp")).reshape(spread.shape)
    down_terms = expert_kernel(x, gain_ffn[None], expert_gate[0], expert_up[0], expert_down[0])
    down_terms = exchanged(down_terms.reshape(plane), ("ep_1", "ep_2", "tp"))
    summed = vmem_call(
        collect_body,
        jax.ShapeDtypeStruct((slots_all, slice_width), BF),
        (down_terms.reshape(spread.shape),),
    )
    returned = exchanged(summed.reshape(n_z, 2 * cores, slice_width), "ep_0")
    returned = returned.reshape(slots_all, slice_width)
    shared = lax.all_gather(parts[:, 1:], "ep_1")
    other = lax.ppermute(shared, "ep_2", [(0, 1), (1, 0)])
    first = lax.axis_index("ep_2") == 0
    shared = jnp.stack([jnp.where(first, shared, other), jnp.where(first, other, shared)])
    shared = shared.transpose(3, 2, 1, 0, 4, 5).reshape(3, model_width, head_dim)
    shared_terms, mix = vmem_call(
        shared_body,
        (
            jax.ShapeDtypeStruct((seq_rows, model_width), BF),
            jax.ShapeDtypeStruct((seq_rows, 128), F32),
        ),
        (mine, gain_ffn[None], w_branch_gate[None], shared[0], shared[1], shared[2]),
        (pltpu.VMEM((seq_rows, model_width), BF),),
    )
    shared_terms = lax.all_gather(shared_terms, "tp")
    shared_terms = lax.dynamic_slice_in_dim(shared_terms, here * slice_width, slice_width, 2)
    shared_out = jnp.sum(shared_terms.astype(F32), axis=0).astype(BF)
    routed = jnp.dot(combine, returned.astype(F32), precision=lax.Precision.HIGHEST)
    branch_sum = routed + mix[:, :1] * shared_out.astype(F32)
    square_part = jnp.sum(branch_sum * branch_sum, axis=1)
    square_total = jnp.sum(to_all(square_part, "tp"), axis=0)
    norm_scale = lax.rsqrt(square_total / model_width + epsilon)
    layer_out = resid.astype(F32) + branch_sum * norm_scale[:, None] * gain_post.astype(F32)
    return (layer_out.astype(BF), new_state)


def solution(mesh):
    torus = Mesh(mesh.devices.reshape(16, 4, 2, mesh.shape["tp"]), ("ep_0", "ep_1", "ep_2", "tp"))
    in_specs = (
        P(EP, None),
        P(EP, "tp", None, None),
        P(None, "tp"),
        P(None, "tp"),
        P(None, "tp"),
        P("tp", None),
        P("tp", None),
        P("tp", EP),
        P(),
        P(),
        P("tp"),
        P(),
        P(EP, "tp"),
        P(EP, "tp"),
        P("tp", EP),
        P(EP, None),
        P(EP, None),
        P(EP, None, "tp"),
        P(EP, None, "tp"),
        P(EP, "tp", None),
    )
    out_specs = (P(EP, "tp"), P(EP, "tp", None, None))

    return jax.shard_map(
        shards, mesh=torus, in_specs=in_specs, out_specs=out_specs, check_vma=False
    )
```

```python
import functools

import jax
import jax.numpy as jnp
from jax import lax
from jax.experimental import pallas as pl
from jax.experimental.pallas import tpu as pltpu
from jax.sharding import Mesh
from jax.sharding import PartitionSpec as P

EP = ("ep_0", "ep_1", "ep_2")
epsilon = 1e-06
BF = jnp.bfloat16
F32 = jnp.float32
NT = (((1,), (1,)), ((), ()))


def exchanged(value, axes):
    return lax.all_to_all(value, axes, 0, 0, tiled=True)


def to_all(value, axes):
    devices = lax.axis_size(axes)
    return exchanged(jnp.broadcast_to(value[None], (devices, *value.shape)), axes)


def turned(value, step, devices):
    if step == 0:
        return value
    return lax.ppermute(value, "tp", [(k, (k + step) % devices) for k in range(devices)])


def rmsnorm(values_in, gain):
    scale = lax.rsqrt(jnp.mean(values_in * values_in, axis=-1, keepdims=True) + epsilon)
    return values_in * scale * gain.astype(F32)


def from_z_order(cores, zs, inverse):
    n = cores * zs * 2
    core_major = lax.broadcasted_iota(jnp.int32, (n, n), 1 if inverse else 0)
    z_major = lax.broadcasted_iota(jnp.int32, (n, n), 0 if inverse else 1)
    core, z, slot = core_major // (2 * zs), (core_major // 2) % zs, core_major % 2
    return jnp.where(z_major == (z * cores + core) * 2 + slot, 1.0, 0.0).astype(BF)


def vmem_call(body, out_shape, args, scratch=(), limit=32):
    vmem = pl.BlockSpec(memory_space=pltpu.VMEM)
    return pl.pallas_call(
        body,
        out_shape=out_shape,
        in_specs=[vmem] * len(args),
        out_specs=jax.tree.map(lambda _: vmem, out_shape),
        scratch_shapes=list(scratch),
        compiler_params=pltpu.CompilerParams(vmem_limit_bytes=limit * 1024 * 1024),
    )(*args)


def project_body(heads, parts, out):
    cores, n_tp, rows, lanes = out.shape
    n_z = parts.shape[0]
    near = n_z // n_tp
    acts = heads[...].reshape(cores * rows, heads.shape[2])
    for t in range(n_tp):
        start = t * near
        other = (t ^ 1) * near
        order = list(range(start, start + near)) + list(range(other, other + near))
        columns = jnp.concatenate([parts[z, 0] for z in order], axis=0)
        term = lax.dot_general(acts, columns, NT, preferred_element_type=F32).astype(BF)
        out[:, t] = term.reshape(cores, rows, lanes)


def dispatch_body(terms, tok, chosen, resid, send, *, piece):
    cores, n_tp, rows, lanes = terms.shape
    parts = []
    for k in range(cores):
        part = terms[k, 0].astype(F32)
        for t in range(1, n_tp):
            part = part + terms[k, t].astype(F32)
        parts.append(part.astype(BF).astype(F32))
    owner = lax.broadcasted_iota(jnp.int32, (rows, lanes), 1) // piece
    for z in range(tok.shape[1] // lanes):
        mixed = jnp.zeros((rows, lanes), F32)
        for k in range(cores):
            turn = (k - z) * piece % lanes
            moved = pltpu.roll(parts[k], turn, 1) if turn else parts[k]
            mixed = jnp.where(owner == k, moved, mixed)
        cols = pl.ds(z * lanes, lanes)
        resid[:, cols] = (tok[:, cols].astype(F32) + mixed).astype(BF)
    send[...] = jnp.dot(chosen[...], resid[...], preferred_element_type=F32).astype(BF)


def spread_body(arrived, out):
    cores, n_tp, rows, width = out.shape
    perm = from_z_order(cores, rows // 2, False)
    moved = jnp.dot(perm, arrived[...], preferred_element_type=F32).astype(BF)
    for t in range(n_tp):
        out[:, t] = moved.reshape(cores, rows, width)


def collect_body(terms, out):
    cores, n_tp, rows, width = terms.shape
    total = terms[:, 0].astype(F32)
    for t in range(1, n_tp):
        total = total + terms[:, t].astype(F32)
    perm = from_z_order(cores, rows // 2, True)
    total = total.astype(BF).reshape(cores * rows, width)
    out[...] = jnp.dot(perm, total, preferred_element_type=F32).astype(BF)


def normed_columns(x, gain, hn):
    slice_width = hn.shape[1] // x[0]
    squares = None
    for j in range(x[0]):
        wide = x[1](j).astype(F32)
        part = jnp.sum(wide * wide, axis=1, keepdims=True)
        squares = part if squares is None else squares + part
    scale = lax.rsqrt(squares / hn.shape[1] + epsilon)
    for j in range(x[0]):
        cols = pl.ds(j * slice_width, slice_width)
        hn[:, cols] = (x[1](j).astype(F32) * scale * gain[:, cols].astype(F32)).astype(BF)


def expert_body(x, gain, gate_hbm, up_hbm, down_hbm, out, hn, gate_w, up_w, down_w, sems):
    cores, n_tp, rows, slice_width = x.shape
    total = cores * rows
    copies = [
        pltpu.make_async_copy(src, dst, sems.at[k])
        for k, (src, dst) in enumerate(
            ((gate_hbm, gate_w), (up_hbm, up_w), (down_hbm, down_w))
        )
    ]
    for copy in copies:
        copy.start()
    normed_columns((n_tp, lambda j: x[:, j].reshape(total, slice_width)), gain, hn)
    copies[0].wait()
    gate_pre = jnp.dot(hn[...], gate_w[...], preferred_element_type=F32)
    copies[1].wait()
    up_pre = jnp.dot(hn[...], up_w[...], preferred_element_type=F32)
    hidden = (gate_pre * jax.nn.sigmoid(gate_pre) * up_pre).astype(BF)
    copies[2].wait()
    for j in range(n_tp):
        cols = pl.ds(j * slice_width, slice_width)
        part = jnp.dot(hidden, down_w[:, cols], preferred_element_type=F32).astype(BF)
        out[:, j] = part.reshape(cores, rows, slice_width)


def expert_kernel(x, gain, gate_w, up_w, down_w):
    cores, n_tp, rows, slice_width = x.shape
    vmem = pl.BlockSpec(memory_space=pltpu.VMEM)
    hbm = pl.BlockSpec(memory_space=pl.ANY)
    return pl.pallas_call(
        expert_body,
        out_shape=jax.ShapeDtypeStruct(x.shape, BF),
        in_specs=[vmem, vmem, hbm, hbm, hbm],
        out_specs=vmem,
        scratch_shapes=[
            pltpu.VMEM((cores * rows, n_tp * slice_width), BF),
            pltpu.VMEM(gate_w.shape, BF),
            pltpu.VMEM(up_w.shape, BF),
            pltpu.VMEM(down_w.shape, BF),
            pltpu.SemaphoreType.DMA((3,)),
        ],
        compiler_params=pltpu.CompilerParams(vmem_limit_bytes=32 * 1024 * 1024),
        name="expert",
    )(x, gain, gate_w, up_w, down_w)


def shared_body(place, x, gain, mix_w, gate_w, up_w, down_w, out, mix):
    n_tp, rows, slice_width = x.shape
    here = place[0]
    squares = jnp.zeros((rows, 1), F32)
    for k in range(n_tp):
        wide = x[k].astype(F32)
        squares = squares + jnp.sum(wide * wide, axis=1, keepdims=True)
    scale = lax.rsqrt(squares / (n_tp * slice_width) + epsilon)
    logits = jnp.zeros((rows, 1), F32)
    gate_pre = jnp.zeros((rows, gate_w.shape[1]), F32)
    up_pre = jnp.zeros((rows, up_w.shape[1]), F32)
    for k in range(n_tp):
        j = lax.rem(here + (n_tp - k), n_tp)
        cols = pl.ds(pl.multiple_of(j * slice_width, slice_width), slice_width)
        part = (x[k].astype(F32) * scale * gain[pl.ds(j, 1), :].astype(F32)).astype(BF)
        logits = logits + jnp.sum(
            part.astype(F32) * mix_w[pl.ds(j, 1), :].astype(F32), axis=1, keepdims=True
        )
        gate_pre = gate_pre + jnp.dot(part, gate_w[cols, :], preferred_element_type=F32)
        up_pre = up_pre + jnp.dot(part, up_w[cols, :], preferred_element_type=F32)
    mix[...] = jnp.broadcast_to(jax.nn.sigmoid(logits), mix.shape)
    hidden = (gate_pre * jax.nn.sigmoid(gate_pre) * up_pre).astype(BF)
    for k in range(n_tp):
        j = lax.rem(here + k, n_tp)
        cols = pl.ds(pl.multiple_of(j * slice_width, slice_width), slice_width)
        out[k] = lax.dot_general(hidden, down_w[cols, :], NT, preferred_element_type=F32).astype(BF)


def shared_kernel(place, *args):
    n_tp, rows, slice_width = args[0].shape
    vmem = pl.BlockSpec(memory_space=pltpu.VMEM)
    smem = pl.BlockSpec(memory_space=pltpu.SMEM)
    return pl.pallas_call(
        shared_body,
        out_shape=(
            jax.ShapeDtypeStruct((n_tp, rows, slice_width), BF),
            jax.ShapeDtypeStruct((rows, 128), F32),
        ),
        in_specs=[smem] + [vmem] * len(args),
        out_specs=(vmem, vmem),
        compiler_params=pltpu.CompilerParams(vmem_limit_bytes=16 * 1024 * 1024),
        name="shared",
    )(place, *args)


def shards(
    tokens,
    carried_state,
    w_query,
    w_forget,
    w_value,
    forget_floor,
    head_gain,
    w_out,
    gain_mix,
    gain_ffn,
    gain_post,
    w_branch_gate,
    shared_gate,
    shared_up,
    shared_down,
    routes,
    route_weights,
    expert_gate,
    expert_up,
    expert_down,
):
    seq_rows, model_width = tokens.shape
    head_dim = carried_state.shape[2]
    n_ep = lax.axis_size(EP)
    n_z = lax.axis_size("ep_0")
    n_tp = lax.axis_size("tp")
    cores = n_ep // n_z
    piece = w_out.shape[1]
    slice_width = model_width // n_tp
    slots_all = 2 * n_ep
    here = lax.axis_index("tp")
    parts = to_all(jnp.stack([w_out.T, shared_gate, shared_up, shared_down.T]), "ep_0")
    column = lax.broadcasted_iota(jnp.int32, (1, 1, slots_all), 2)
    hits = routes[:, :, None] == column // 2
    named = jnp.any(hits, axis=1).astype(BF)
    tri = (
        lax.broadcasted_iota(jnp.int32, (seq_rows, seq_rows), 0)
        > lax.broadcasted_iota(jnp.int32, (seq_rows, seq_rows), 1)
    ).astype(BF)
    rank = jnp.dot(tri, named, preferred_element_type=F32)
    taken = (named > 0) & (rank == (column[0] % 2).astype(F32))
    chosen = jnp.where(taken, 1.0, 0.0).astype(BF).T
    combine = jnp.where(taken, jnp.sum(jnp.where(hits, route_weights[:, :, None], 0.0), axis=1), 0.0)
    normed = rmsnorm(tokens.astype(F32), gain_mix).astype(BF)
    queries = jax.nn.silu(jnp.dot(normed, w_query, preferred_element_type=F32))
    forget_pre = jnp.dot(normed, w_forget, preferred_element_type=F32)
    values_in = jnp.dot(normed, w_value, preferred_element_type=F32)
    queries = queries.reshape(seq_rows, 1, head_dim)
    forget_pre = forget_pre.reshape(seq_rows, 1, head_dim)
    values_in = values_in.reshape(seq_rows, 1, head_dim)
    forget = forget_floor + (1.0 - forget_floor) * jax.nn.sigmoid(forget_pre)
    keys_in = (1.0 - forget_floor) * jax.nn.sigmoid(-forget_pre)
    new_state = forget[..., None] * carried_state + keys_in[..., None] * values_in[:, :, None, :]
    readout = jnp.einsum("bhd,bhdv->bhv", queries, new_state, precision=lax.Precision.HIGHEST)
    head_out = rmsnorm(readout, head_gain).astype(BF).reshape(seq_rows, head_dim)
    head_out, parts = lax.optimization_barrier((head_out, parts))
    heads = to_all(head_out, ("ep_1", "ep_2"))
    terms = vmem_call(
        project_body, jax.ShapeDtypeStruct((cores, n_tp, seq_rows, 128), BF), (heads, parts)
    )
    terms = exchanged(
        terms.reshape(cores * n_tp, seq_rows, 128), ("ep_1", "ep_2", "tp")
    ).reshape(terms.shape)
    token_slice = lax.dynamic_slice_in_dim(tokens, here * slice_width, slice_width, 1)
    resid, send = vmem_call(
        functools.partial(dispatch_body, piece=piece),
        (
            jax.ShapeDtypeStruct((seq_rows, slice_width), BF),
            jax.ShapeDtypeStruct((slots_all, slice_width), BF),
        ),
        (terms, token_slice, chosen),
    )
    arrived = exchanged(send.reshape(n_z, 2 * cores, slice_width), "ep_0")
    mine = jnp.stack([turned(resid, k, n_tp) for k in range(n_tp)])
    spread = vmem_call(
        spread_body,
        jax.ShapeDtypeStruct((cores, n_tp, 2 * n_z, slice_width), BF),
        (arrived.reshape(slots_all, slice_width),),
    )
    plane = (cores * n_tp, 2 * n_z, slice_width)
    x = exchanged(spread.reshape(plane), ("ep_1", "ep_2", "tp")).reshape(spread.shape)
    down_terms = expert_kernel(x, gain_ffn[None], expert_gate[0], expert_up[0], expert_down[0])
    down_terms = exchanged(down_terms.reshape(plane), ("ep_1", "ep_2", "tp"))
    summed = vmem_call(
        collect_body,
        jax.ShapeDtypeStruct((slots_all, slice_width), BF),
        (down_terms.reshape(spread.shape),),
    )
    returned = exchanged(summed.reshape(n_z, 2 * cores, slice_width), "ep_0")
    returned = returned.reshape(slots_all, slice_width)
    shared = lax.all_gather(parts[:, 1:], "ep_1")
    other = lax.ppermute(shared, "ep_2", [(0, 1), (1, 0)])
    first = lax.axis_index("ep_2") == 0
    shared = jnp.stack([jnp.where(first, shared, other), jnp.where(first, other, shared)])
    shared = shared.transpose(3, 2, 1, 0, 4, 5).reshape(3, model_width, head_dim)
    shared_terms, mix = shared_kernel(
        here.astype(jnp.int32)[None],
        mine,
        gain_ffn.reshape(n_tp, slice_width).astype(F32),
        w_branch_gate.reshape(n_tp, slice_width).astype(F32),
        shared[0],
        shared[1],
        shared[2],
    )
    shared_parts = [turned(shared_terms[k], k, n_tp) for k in range(n_tp)]
    shared_out = sum(p.astype(F32) for p in shared_parts).astype(BF)
    routed = jnp.dot(combine, returned.astype(F32), precision=lax.Precision.HIGHEST)
    branch_sum = routed + mix[:, :1] * shared_out.astype(F32)
    square_part = jnp.sum(branch_sum * branch_sum, axis=1)
    square_total = jnp.sum(to_all(square_part, "tp"), axis=0)
    norm_scale = lax.rsqrt(square_total / model_width + epsilon)
    layer_out = resid.astype(F32) + branch_sum * norm_scale[:, None] * gain_post.astype(F32)
    return (layer_out.astype(BF), new_state)


def solution(mesh):
    torus = Mesh(mesh.devices.reshape(16, 4, 2, mesh.shape["tp"]), ("ep_0", "ep_1", "ep_2", "tp"))
    in_specs = (
        P(EP, None),
        P(EP, "tp", None, None),
        P(None, "tp"),
        P(None, "tp"),
        P(None, "tp"),
        P("tp", None),
        P("tp", None),
        P("tp", EP),
        P(),
        P(),
        P("tp"),
        P(),
        P(EP, "tp"),
        P(EP, "tp"),
        P("tp", EP),
        P(EP, None),
        P(EP, None),
        P(EP, None, "tp"),
        P(EP, None, "tp"),
        P(EP, "tp", None),
    )
    out_specs = (P(EP, "tp"), P(EP, "tp", None, None))

    return jax.shard_map(
        shards, mesh=torus, in_specs=in_specs, out_specs=out_specs, check_vma=False
    )
```

```python
import functools

import jax
import jax.numpy as jnp
from jax import lax
from jax.experimental import pallas as pl
from jax.experimental.pallas import tpu as pltpu
from jax.sharding import Mesh
from jax.sharding import PartitionSpec as P

EP = ("ep_0", "ep_1", "ep_2")
epsilon = 1e-06
BF = jnp.bfloat16
F32 = jnp.float32
NT = (((1,), (1,)), ((), ()))


def exchanged(value, axes):
    return lax.all_to_all(value, axes, 0, 0, tiled=True)


def to_all(value, axes):
    devices = lax.axis_size(axes)
    return exchanged(jnp.broadcast_to(value[None], (devices, *value.shape)), axes)


def turned(value, step, devices):
    if step == 0:
        return value
    return lax.ppermute(value, "tp", [(k, (k + step) % devices) for k in range(devices)])


def rmsnorm(values_in, gain):
    scale = lax.rsqrt(jnp.mean(values_in * values_in, axis=-1, keepdims=True) + epsilon)
    return values_in * scale * gain.astype(F32)


def from_z_order(cores, zs, inverse):
    n = cores * zs * 2
    core_major = lax.broadcasted_iota(jnp.int32, (n, n), 1 if inverse else 0)
    z_major = lax.broadcasted_iota(jnp.int32, (n, n), 0 if inverse else 1)
    core, z, slot = core_major // (2 * zs), (core_major // 2) % zs, core_major % 2
    return jnp.where(z_major == (z * cores + core) * 2 + slot, 1.0, 0.0).astype(BF)


def vmem_call(body, out_shape, args, scratch=(), limit=32):
    vmem = pl.BlockSpec(memory_space=pltpu.VMEM)
    return pl.pallas_call(
        body,
        out_shape=out_shape,
        in_specs=[vmem] * len(args),
        out_specs=jax.tree.map(lambda _: vmem, out_shape),
        scratch_shapes=list(scratch),
        compiler_params=pltpu.CompilerParams(vmem_limit_bytes=limit * 1024 * 1024),
    )(*args)


def project_body(heads, parts, out):
    cores, n_tp, rows, lanes = out.shape
    n_z = parts.shape[0]
    near = n_z // n_tp
    acts = heads[...].reshape(cores * rows, heads.shape[2])
    for t in range(n_tp):
        start = t * near
        other = (t ^ 1) * near
        order = list(range(start, start + near)) + list(range(other, other + near))
        columns = jnp.concatenate([parts[z, 0] for z in order], axis=0)
        term = lax.dot_general(acts, columns, NT, preferred_element_type=F32).astype(BF)
        out[:, t] = term.reshape(cores, rows, lanes)


def dispatch_body(terms, tok, chosen, resid, send, *, piece):
    cores, n_tp, rows, lanes = terms.shape
    parts = []
    for k in range(cores):
        part = terms[k, 0].astype(F32)
        for t in range(1, n_tp):
            part = part + terms[k, t].astype(F32)
        parts.append(part.astype(BF).astype(F32))
    owner = lax.broadcasted_iota(jnp.int32, (rows, lanes), 1) // piece
    for z in range(tok.shape[1] // lanes):
        mixed = jnp.zeros((rows, lanes), F32)
        for k in range(cores):
            turn = (k - z) * piece % lanes
            moved = pltpu.roll(parts[k], turn, 1) if turn else parts[k]
            mixed = jnp.where(owner == k, moved, mixed)
        cols = pl.ds(z * lanes, lanes)
        resid[:, cols] = (tok[:, cols].astype(F32) + mixed).astype(BF)
    send[...] = jnp.dot(chosen[...], resid[...], preferred_element_type=F32).astype(BF)


def spread_body(arrived, out):
    cores, n_tp, rows, width = out.shape
    perm = from_z_order(cores, rows // 2, False)
    moved = jnp.dot(perm, arrived[...], preferred_element_type=F32).astype(BF)
    for t in range(n_tp):
        out[:, t] = moved.reshape(cores, rows, width)


def combine_body(weights, returned, shared, mix, branch, squares):
    rest = weights[...]
    total = mix[:, :1] * shared[...].astype(F32)
    for _ in range(3):
        part = rest.astype(BF)
        rest = rest - part.astype(F32)
        total = total + jnp.dot(part, returned[...], preferred_element_type=F32)
    branch[...] = total
    square = jnp.sum(total * total, axis=1, keepdims=True)
    squares[...] = jnp.broadcast_to(square[None], squares.shape)


def collect_body(terms, first, second, third, fourth, out, shared):
    parts = [r[...].astype(F32) for r in (first, second, third, fourth)]
    shared[...] = (parts[0] + parts[1] + parts[2] + parts[3]).astype(BF)
    cores, n_tp, rows, width = terms.shape
    total = terms[:, 0].astype(F32)
    for t in range(1, n_tp):
        total = total + terms[:, t].astype(F32)
    perm = from_z_order(cores, rows // 2, True)
    total = total.astype(BF).reshape(cores * rows, width)
    out[...] = jnp.dot(perm, total, preferred_element_type=F32).astype(BF)


def normed_columns(x, gain, hn):
    slice_width = hn.shape[1] // x[0]
    squares = None
    for j in range(x[0]):
        wide = x[1](j).astype(F32)
        part = jnp.sum(wide * wide, axis=1, keepdims=True)
        squares = part if squares is None else squares + part
    scale = lax.rsqrt(squares / hn.shape[1] + epsilon)
    for j in range(x[0]):
        cols = pl.ds(j * slice_width, slice_width)
        hn[:, cols] = (x[1](j).astype(F32) * scale * gain[:, cols].astype(F32)).astype(BF)


def expert_body(
    x, gain, gate_hbm, up_hbm, down_hbm, out, hn, gate_w, up_w, down_w, held, sems, sent
):
    cores, n_tp, rows, slice_width = x.shape
    total = cores * rows
    copies = [
        pltpu.make_async_copy(src, dst, sems.at[k])
        for k, (src, dst) in enumerate(
            ((gate_hbm, gate_w), (up_hbm, up_w), (down_hbm, down_w))
        )
    ]
    for copy in copies:
        copy.start()
    normed_columns((n_tp, lambda j: x[:, j].reshape(total, slice_width)), gain, hn)
    copies[0].wait()
    gate_pre = jnp.dot(hn[...], gate_w[...], preferred_element_type=F32)
    copies[1].wait()
    up_pre = jnp.dot(hn[...], up_w[...], preferred_element_type=F32)
    hidden = (gate_pre * jax.nn.sigmoid(gate_pre) * up_pre).astype(BF)
    copies[2].wait()
    for j in range(n_tp):
        cols = pl.ds(j * slice_width, slice_width)
        part = jnp.dot(hidden, down_w[:, cols], preferred_element_type=F32).astype(BF)
        held[j] = part.reshape(cores, rows, slice_width)
        copies.append(pltpu.make_async_copy(held.at[j], out.at[:, j], sent.at[j]))
        copies[-1].start()
    for copy in copies[3:]:
        copy.wait()


def expert_kernel(x, gain, gate_w, up_w, down_w):
    cores, n_tp, rows, slice_width = x.shape
    vmem = pl.BlockSpec(memory_space=pltpu.VMEM)
    hbm = pl.BlockSpec(memory_space=pl.ANY)
    return pl.pallas_call(
        expert_body,
        out_shape=jax.ShapeDtypeStruct(x.shape, BF),
        in_specs=[vmem, vmem, hbm, hbm, hbm],
        out_specs=hbm,
        scratch_shapes=[
            pltpu.VMEM((cores * rows, n_tp * slice_width), BF),
            pltpu.VMEM(gate_w.shape, BF),
            pltpu.VMEM(up_w.shape, BF),
            pltpu.VMEM(down_w.shape, BF),
            pltpu.VMEM((n_tp, cores, rows, slice_width), BF),
            pltpu.SemaphoreType.DMA((3,)),
            pltpu.SemaphoreType.DMA((n_tp,)),
        ],
        compiler_params=pltpu.CompilerParams(vmem_limit_bytes=32 * 1024 * 1024),
        name="expert",
    )(x, gain, gate_w, up_w, down_w)


def shared_body(place, x, gain, mix_w, gate_w, up_w, down_w, out, mix):
    n_tp, rows, slice_width = x.shape
    here = place[0]
    squares = jnp.zeros((rows, 1), F32)
    for k in range(n_tp):
        wide = x[k].astype(F32)
        squares = squares + jnp.sum(wide * wide, axis=1, keepdims=True)
    scale = lax.rsqrt(squares / (n_tp * slice_width) + epsilon)
    logits = jnp.zeros((rows, 1), F32)
    gate_pre = jnp.zeros((rows, gate_w.shape[1]), F32)
    up_pre = jnp.zeros((rows, up_w.shape[1]), F32)
    for k in range(n_tp):
        j = lax.rem(here + (n_tp - k), n_tp)
        cols = pl.ds(pl.multiple_of(j * slice_width, slice_width), slice_width)
        part = (x[k].astype(F32) * scale * gain[pl.ds(j, 1), :].astype(F32)).astype(BF)
        logits = logits + jnp.sum(
            part.astype(F32) * mix_w[pl.ds(j, 1), :].astype(F32), axis=1, keepdims=True
        )
        gate_pre = gate_pre + jnp.dot(part, gate_w[cols, :], preferred_element_type=F32)
        up_pre = up_pre + jnp.dot(part, up_w[cols, :], preferred_element_type=F32)
    mix[...] = jnp.broadcast_to(jax.nn.sigmoid(logits), mix.shape)
    hidden = (gate_pre * jax.nn.sigmoid(gate_pre) * up_pre).astype(BF)
    for k in range(n_tp):
        j = lax.rem(here + k, n_tp)
        cols = pl.ds(pl.multiple_of(j * slice_width, slice_width), slice_width)
        out[k] = lax.dot_general(hidden, down_w[cols, :], NT, preferred_element_type=F32).astype(BF)


def shared_kernel(place, *args):
    n_tp, rows, slice_width = args[0].shape
    vmem = pl.BlockSpec(memory_space=pltpu.VMEM)
    smem = pl.BlockSpec(memory_space=pltpu.SMEM)
    return pl.pallas_call(
        shared_body,
        out_shape=(
            jax.ShapeDtypeStruct((n_tp, rows, slice_width), BF),
            jax.ShapeDtypeStruct((rows, 128), F32),
        ),
        in_specs=[smem] + [vmem] * len(args),
        out_specs=(vmem, vmem),
        compiler_params=pltpu.CompilerParams(vmem_limit_bytes=16 * 1024 * 1024),
        name="shared",
    )(place, *args)


def shards(
    tokens,
    carried_state,
    w_query,
    w_forget,
    w_value,
    forget_floor,
    head_gain,
    w_out,
    gain_mix,
    gain_ffn,
    gain_post,
    w_branch_gate,
    shared_gate,
    shared_up,
    shared_down,
    routes,
    route_weights,
    expert_gate,
    expert_up,
    expert_down,
):
    seq_rows, model_width = tokens.shape
    head_dim = carried_state.shape[2]
    n_ep = lax.axis_size(EP)
    n_z = lax.axis_size("ep_0")
    n_tp = lax.axis_size("tp")
    cores = n_ep // n_z
    piece = w_out.shape[1]
    slice_width = model_width // n_tp
    slots_all = 2 * n_ep
    here = lax.axis_index("tp")
    parts = to_all(jnp.stack([w_out.T, shared_gate, shared_up, shared_down.T]), "ep_0")
    column = lax.broadcasted_iota(jnp.int32, (1, 1, slots_all), 2)
    hits = routes[:, :, None] == column // 2
    named = jnp.any(hits, axis=1).astype(BF)
    tri = (
        lax.broadcasted_iota(jnp.int32, (seq_rows, seq_rows), 0)
        > lax.broadcasted_iota(jnp.int32, (seq_rows, seq_rows), 1)
    ).astype(BF)
    rank = jnp.dot(tri, named, preferred_element_type=F32)
    taken = (named > 0) & (rank == (column[0] % 2).astype(F32))
    chosen = jnp.where(taken, 1.0, 0.0).astype(BF).T
    combine = jnp.where(hits, route_weights[:, :, None], 0.0)
    combine = jnp.where(taken, jnp.sum(combine, axis=1), 0.0)
    normed = rmsnorm(tokens.astype(F32), gain_mix).astype(BF)
    queries = jax.nn.silu(jnp.dot(normed, w_query, preferred_element_type=F32))
    forget_pre = jnp.dot(normed, w_forget, preferred_element_type=F32)
    values_in = jnp.dot(normed, w_value, preferred_element_type=F32)
    queries = queries.reshape(seq_rows, 1, head_dim)
    forget_pre = forget_pre.reshape(seq_rows, 1, head_dim)
    values_in = values_in.reshape(seq_rows, 1, head_dim)
    forget = forget_floor + (1.0 - forget_floor) * jax.nn.sigmoid(forget_pre)
    keys_in = (1.0 - forget_floor) * jax.nn.sigmoid(-forget_pre)
    new_state = forget[..., None] * carried_state + keys_in[..., None] * values_in[:, :, None, :]
    readout = jnp.einsum("bhd,bhdv->bhv", queries, new_state, precision=lax.Precision.HIGHEST)
    head_out = rmsnorm(readout, head_gain).astype(BF).reshape(seq_rows, head_dim)
    heads = jnp.broadcast_to(head_out[None], (cores, seq_rows, head_dim))
    heads, parts = lax.optimization_barrier((heads, parts))
    heads = exchanged(heads, ("ep_1", "ep_2"))
    terms = vmem_call(
        project_body, jax.ShapeDtypeStruct((cores, n_tp, seq_rows, 128), BF), (heads, parts)
    )
    terms = exchanged(
        terms.reshape(cores * n_tp, seq_rows, 128), ("ep_1", "ep_2", "tp")
    ).reshape(terms.shape)
    token_slice = lax.dynamic_slice_in_dim(tokens, here * slice_width, slice_width, 1)
    resid, send = vmem_call(
        functools.partial(dispatch_body, piece=piece),
        (
            jax.ShapeDtypeStruct((seq_rows, slice_width), BF),
            jax.ShapeDtypeStruct((slots_all, slice_width), BF),
        ),
        (terms, token_slice, chosen),
    )
    arrived = exchanged(send.reshape(n_z, 2 * cores, slice_width), "ep_0")
    mine = jnp.stack([turned(resid, k, n_tp) for k in range(n_tp)])
    spread = vmem_call(
        spread_body,
        jax.ShapeDtypeStruct((cores, n_tp, 2 * n_z, slice_width), BF),
        (arrived.reshape(slots_all, slice_width),),
    )
    plane = (cores * n_tp, 2 * n_z, slice_width)
    x = exchanged(spread.reshape(plane), ("ep_1", "ep_2", "tp")).reshape(spread.shape)
    down_terms = expert_kernel(x, gain_ffn[None], expert_gate[0], expert_up[0], expert_down[0])
    down_terms = exchanged(down_terms.reshape(plane), ("ep_1", "ep_2", "tp"))
    shared = lax.all_gather(parts[:, 1:], "ep_1")
    other = lax.ppermute(shared, "ep_2", [(0, 1), (1, 0)])
    first = lax.axis_index("ep_2") == 0
    shared = jnp.stack([jnp.where(first, shared, other), jnp.where(first, other, shared)])
    shared = shared.transpose(3, 2, 1, 0, 4, 5).reshape(3, model_width, head_dim)
    shared_terms, mix = shared_kernel(
        here.astype(jnp.int32)[None],
        mine,
        gain_ffn.reshape(n_tp, slice_width).astype(F32),
        w_branch_gate.reshape(n_tp, slice_width).astype(F32),
        shared[0],
        shared[1],
        shared[2],
    )
    shared_parts = [turned(shared_terms[k], k, n_tp) for k in range(n_tp)]
    summed, shared_out = vmem_call(
        collect_body,
        (
            jax.ShapeDtypeStruct((slots_all, slice_width), BF),
            jax.ShapeDtypeStruct((seq_rows, slice_width), BF),
        ),
        (down_terms.reshape(spread.shape), *shared_parts),
    )
    returned = exchanged(summed.reshape(n_z, 2 * cores, slice_width), "ep_0")
    returned = returned.reshape(slots_all, slice_width)
    branch_sum, squares = vmem_call(
        combine_body,
        (
            jax.ShapeDtypeStruct((seq_rows, slice_width), F32),
            jax.ShapeDtypeStruct((n_tp, seq_rows, 128), F32),
        ),
        (combine, returned, shared_out, mix),
    )
    square_total = jnp.sum(exchanged(squares, "tp")[:, :, 0], axis=0)
    norm_scale = lax.rsqrt(square_total / model_width + epsilon)
    layer_out = resid.astype(F32) + branch_sum * norm_scale[:, None] * gain_post.astype(F32)
    return (layer_out.astype(BF), new_state)


def solution(mesh):
    torus = Mesh(mesh.devices.reshape(16, 4, 2, mesh.shape["tp"]), ("ep_0", "ep_1", "ep_2", "tp"))
    in_specs = (
        P(EP, None),
        P(EP, "tp", None, None),
        P(None, "tp"),
        P(None, "tp"),
        P(None, "tp"),
        P("tp", None),
        P("tp", None),
        P("tp", EP),
        P(),
        P(),
        P("tp"),
        P(),
        P(EP, "tp"),
        P(EP, "tp"),
        P("tp", EP),
        P(EP, None),
        P(EP, None),
        P(EP, None, "tp"),
        P(EP, None, "tp"),
        P(EP, "tp", None),
    )
    out_specs = (P(EP, "tp"), P(EP, "tp", None, None))

    return jax.shard_map(
        shards, mesh=torus, in_specs=in_specs, out_specs=out_specs, check_vma=False
    )
```

```python
import functools

import jax
import jax.numpy as jnp
from jax import lax
from jax.experimental import pallas as pl
from jax.experimental.pallas import tpu as pltpu
from jax.sharding import Mesh
from jax.sharding import PartitionSpec as P

EP = ("ep_0", "ep_1", "ep_2")
epsilon = 1e-06
BF = jnp.bfloat16
F32 = jnp.float32
NT = (((1,), (1,)), ((), ()))


def exchanged(value, axes):
    return lax.all_to_all(value, axes, 0, 0, tiled=True)


def to_all(value, axes):
    devices = lax.axis_size(axes)
    return exchanged(jnp.broadcast_to(value[None], (devices, *value.shape)), axes)


def turned(value, step, devices):
    if step == 0:
        return value
    return lax.ppermute(value, "tp", [(k, (k + step) % devices) for k in range(devices)])


def rmsnorm(values_in, gain):
    scale = lax.rsqrt(jnp.mean(values_in * values_in, axis=-1, keepdims=True) + epsilon)
    return values_in * scale * gain.astype(F32)


def from_z_order(cores, zs, inverse):
    n = cores * zs * 2
    core_major = lax.broadcasted_iota(jnp.int32, (n, n), 1 if inverse else 0)
    z_major = lax.broadcasted_iota(jnp.int32, (n, n), 0 if inverse else 1)
    core, z, slot = core_major // (2 * zs), (core_major // 2) % zs, core_major % 2
    return jnp.where(z_major == (z * cores + core) * 2 + slot, 1.0, 0.0).astype(BF)


def vmem_call(body, out_shape, args, scratch=(), limit=32):
    vmem = pl.BlockSpec(memory_space=pltpu.VMEM)
    return pl.pallas_call(
        body,
        out_shape=out_shape,
        in_specs=[vmem] * len(args),
        out_specs=jax.tree.map(lambda _: vmem, out_shape),
        scratch_shapes=list(scratch),
        compiler_params=pltpu.CompilerParams(vmem_limit_bytes=limit * 1024 * 1024),
    )(*args)


def project_body(heads, parts, out):
    cores, n_tp, rows, lanes = out.shape
    n_z = parts.shape[0]
    near = n_z // n_tp
    acts = heads[...].reshape(cores * rows, heads.shape[2])
    for t in range(n_tp):
        start = t * near
        other = (t ^ 1) * near
        order = list(range(start, start + near)) + list(range(other, other + near))
        columns = jnp.concatenate([parts[z, 0] for z in order], axis=0)
        term = lax.dot_general(acts, columns, NT, preferred_element_type=F32).astype(BF)
        out[:, t] = term.reshape(cores, rows, lanes)


def dispatch_body(terms, tok, chosen, resid, send, *, piece):
    cores, n_tp, rows, lanes = terms.shape
    parts = []
    for k in range(cores):
        part = terms[k, 0].astype(F32)
        for t in range(1, n_tp):
            part = part + terms[k, t].astype(F32)
        parts.append(part.astype(BF).astype(F32))
    owner = lax.broadcasted_iota(jnp.int32, (rows, lanes), 1) // piece
    for z in range(tok.shape[1] // lanes):
        mixed = jnp.zeros((rows, lanes), F32)
        for k in range(cores):
            turn = (k - z) * piece % lanes
            moved = pltpu.roll(parts[k], turn, 1) if turn else parts[k]
            mixed = jnp.where(owner == k, moved, mixed)
        cols = pl.ds(z * lanes, lanes)
        resid[:, cols] = (tok[:, cols].astype(F32) + mixed).astype(BF)
    send[...] = jnp.dot(chosen[...], resid[...], preferred_element_type=F32).astype(BF)


def spread_body(arrived, out):
    cores, n_tp, rows, width = out.shape
    perm = from_z_order(cores, rows // 2, False)
    moved = jnp.dot(perm, arrived[...], preferred_element_type=F32).astype(BF)
    for t in range(n_tp):
        out[:, t] = moved.reshape(cores, rows, width)


def combine_body(weights, returned, shared, mix, branch, squares):
    rest = weights[...]
    total = mix[:, :1] * shared[...].astype(F32)
    for _ in range(3):
        part = rest.astype(BF)
        rest = rest - part.astype(F32)
        total = total + jnp.dot(part, returned[...], preferred_element_type=F32)
    branch[...] = total
    square = jnp.sum(total * total, axis=1, keepdims=True)
    group = lax.broadcasted_iota(jnp.int32, squares.shape[1:], 1)
    packed = jnp.zeros(squares.shape[1:], F32)
    for g in range(total.shape[0] // 8):
        packed = jnp.where(group == g, square[8 * g : 8 * g + 8], packed)
    squares[...] = jnp.broadcast_to(packed[None], squares.shape)


def final_body(squares, branch, resid, gain, out):
    n_tp = squares.shape[0]
    total = squares[0]
    for t in range(1, n_tp):
        total = total + squares[t]
    scale = lax.rsqrt(total / (n_tp * out.shape[1]) + epsilon)
    for g in range(out.shape[0] // 8):
        rows = pl.ds(8 * g, 8)
        grown = branch[rows, :] * scale[:, g : g + 1] * gain[...]
        out[rows, :] = (resid[rows, :].astype(F32) + grown).astype(BF)


def collect_body(terms, first, second, third, fourth, out, shared):
    parts = [r[...].astype(F32) for r in (first, second, third, fourth)]
    shared[...] = (parts[0] + parts[1] + parts[2] + parts[3]).astype(BF)
    cores, n_tp, rows, width = terms.shape
    total = terms[:, 0].astype(F32)
    for t in range(1, n_tp):
        total = total + terms[:, t].astype(F32)
    perm = from_z_order(cores, rows // 2, True)
    total = total.astype(BF).reshape(cores * rows, width)
    out[...] = jnp.dot(perm, total, preferred_element_type=F32).astype(BF)


def normed_columns(x, gain, hn):
    slice_width = hn.shape[1] // x[0]
    squares = None
    for j in range(x[0]):
        wide = x[1](j).astype(F32)
        part = jnp.sum(wide * wide, axis=1, keepdims=True)
        squares = part if squares is None else squares + part
    scale = lax.rsqrt(squares / hn.shape[1] + epsilon)
    for j in range(x[0]):
        cols = pl.ds(j * slice_width, slice_width)
        hn[:, cols] = (x[1](j).astype(F32) * scale * gain[:, cols].astype(F32)).astype(BF)


def expert_body(
    x, gain, gate_hbm, up_hbm, down_hbm, out, hn, gate_w, up_w, down_w, held, sems, sent
):
    cores, n_tp, rows, slice_width = x.shape
    total = cores * rows
    copies = [
        pltpu.make_async_copy(src, dst, sems.at[k])
        for k, (src, dst) in enumerate(
            ((gate_hbm, gate_w), (up_hbm, up_w), (down_hbm, down_w))
        )
    ]
    for copy in copies:
        copy.start()
    normed_columns((n_tp, lambda j: x[:, j].reshape(total, slice_width)), gain, hn)
    copies[0].wait()
    gate_pre = jnp.dot(hn[...], gate_w[...], preferred_element_type=F32)
    copies[1].wait()
    up_pre = jnp.dot(hn[...], up_w[...], preferred_element_type=F32)
    hidden = (gate_pre * jax.nn.sigmoid(gate_pre) * up_pre).astype(BF)
    copies[2].wait()
    for j in range(n_tp):
        cols = pl.ds(j * slice_width, slice_width)
        part = jnp.dot(hidden, down_w[:, cols], preferred_element_type=F32).astype(BF)
        held[j] = part.reshape(cores, rows, slice_width)
        copies.append(pltpu.make_async_copy(held.at[j], out.at[:, j], sent.at[j]))
        copies[-1].start()
    for copy in copies[3:]:
        copy.wait()


def expert_kernel(x, gain, gate_w, up_w, down_w):
    cores, n_tp, rows, slice_width = x.shape
    vmem = pl.BlockSpec(memory_space=pltpu.VMEM)
    hbm = pl.BlockSpec(memory_space=pl.ANY)
    return pl.pallas_call(
        expert_body,
        out_shape=jax.ShapeDtypeStruct(x.shape, BF),
        in_specs=[vmem, vmem, hbm, hbm, hbm],
        out_specs=hbm,
        scratch_shapes=[
            pltpu.VMEM((cores * rows, n_tp * slice_width), BF),
            pltpu.VMEM(gate_w.shape, BF),
            pltpu.VMEM(up_w.shape, BF),
            pltpu.VMEM(down_w.shape, BF),
            pltpu.VMEM((n_tp, cores, rows, slice_width), BF),
            pltpu.SemaphoreType.DMA((3,)),
            pltpu.SemaphoreType.DMA((n_tp,)),
        ],
        compiler_params=pltpu.CompilerParams(vmem_limit_bytes=32 * 1024 * 1024),
        name="expert",
    )(x, gain, gate_w, up_w, down_w)


def shared_body(place, x, gain, mix_w, gate_w, up_w, down_w, out, mix):
    n_tp, rows, slice_width = x.shape
    here = place[0]
    squares = jnp.zeros((rows, 1), F32)
    for k in range(n_tp):
        wide = x[k].astype(F32)
        squares = squares + jnp.sum(wide * wide, axis=1, keepdims=True)
    scale = lax.rsqrt(squares / (n_tp * slice_width) + epsilon)
    logits = jnp.zeros((rows, 1), F32)
    gate_pre = jnp.zeros((rows, gate_w.shape[1]), F32)
    up_pre = jnp.zeros((rows, up_w.shape[1]), F32)
    for k in range(n_tp):
        j = lax.rem(here + (n_tp - k), n_tp)
        cols = pl.ds(pl.multiple_of(j * slice_width, slice_width), slice_width)
        part = (x[k].astype(F32) * scale * gain[pl.ds(j, 1), :].astype(F32)).astype(BF)
        logits = logits + jnp.sum(
            part.astype(F32) * mix_w[pl.ds(j, 1), :].astype(F32), axis=1, keepdims=True
        )
        gate_pre = gate_pre + jnp.dot(part, gate_w[cols, :], preferred_element_type=F32)
        up_pre = up_pre + jnp.dot(part, up_w[cols, :], preferred_element_type=F32)
    mix[...] = jnp.broadcast_to(jax.nn.sigmoid(logits), mix.shape)
    hidden = (gate_pre * jax.nn.sigmoid(gate_pre) * up_pre).astype(BF)
    for k in range(n_tp):
        j = lax.rem(here + k, n_tp)
        cols = pl.ds(pl.multiple_of(j * slice_width, slice_width), slice_width)
        out[k] = lax.dot_general(hidden, down_w[cols, :], NT, preferred_element_type=F32).astype(BF)


def shared_kernel(place, *args):
    n_tp, rows, slice_width = args[0].shape
    vmem = pl.BlockSpec(memory_space=pltpu.VMEM)
    smem = pl.BlockSpec(memory_space=pltpu.SMEM)
    return pl.pallas_call(
        shared_body,
        out_shape=(
            jax.ShapeDtypeStruct((n_tp, rows, slice_width), BF),
            jax.ShapeDtypeStruct((rows, 128), F32),
        ),
        in_specs=[smem] + [vmem] * len(args),
        out_specs=(vmem, vmem),
        compiler_params=pltpu.CompilerParams(vmem_limit_bytes=16 * 1024 * 1024),
        name="shared",
    )(place, *args)


def shards(
    tokens,
    carried_state,
    w_query,
    w_forget,
    w_value,
    forget_floor,
    head_gain,
    w_out,
    gain_mix,
    gain_ffn,
    gain_post,
    w_branch_gate,
    shared_gate,
    shared_up,
    shared_down,
    routes,
    route_weights,
    expert_gate,
    expert_up,
    expert_down,
):
    seq_rows, model_width = tokens.shape
    head_dim = carried_state.shape[2]
    n_ep = lax.axis_size(EP)
    n_z = lax.axis_size("ep_0")
    n_tp = lax.axis_size("tp")
    cores = n_ep // n_z
    piece = w_out.shape[1]
    slice_width = model_width // n_tp
    slots_all = 2 * n_ep
    here = lax.axis_index("tp")
    parts = to_all(jnp.stack([w_out.T, shared_gate, shared_up, shared_down.T]), "ep_0")
    column = lax.broadcasted_iota(jnp.int32, (1, 1, slots_all), 2)
    hits = routes[:, :, None] == column // 2
    named = jnp.any(hits, axis=1).astype(BF)
    tri = (
        lax.broadcasted_iota(jnp.int32, (seq_rows, seq_rows), 0)
        > lax.broadcasted_iota(jnp.int32, (seq_rows, seq_rows), 1)
    ).astype(BF)
    rank = jnp.dot(tri, named, preferred_element_type=F32)
    taken = (named > 0) & (rank == (column[0] % 2).astype(F32))
    chosen = jnp.where(taken, 1.0, 0.0).astype(BF).T
    combine = jnp.where(hits, route_weights[:, :, None], 0.0)
    combine = jnp.where(taken, jnp.sum(combine, axis=1), 0.0)
    normed = rmsnorm(tokens.astype(F32), gain_mix).astype(BF)
    queries = jax.nn.silu(jnp.dot(normed, w_query, preferred_element_type=F32))
    forget_pre = jnp.dot(normed, w_forget, preferred_element_type=F32)
    values_in = jnp.dot(normed, w_value, preferred_element_type=F32)
    queries = queries.reshape(seq_rows, 1, head_dim)
    forget_pre = forget_pre.reshape(seq_rows, 1, head_dim)
    values_in = values_in.reshape(seq_rows, 1, head_dim)
    forget = forget_floor + (1.0 - forget_floor) * jax.nn.sigmoid(forget_pre)
    keys_in = (1.0 - forget_floor) * jax.nn.sigmoid(-forget_pre)
    new_state = forget[..., None] * carried_state + keys_in[..., None] * values_in[:, :, None, :]
    readout = jnp.einsum("bhd,bhdv->bhv", queries, new_state, precision=lax.Precision.HIGHEST)
    head_out = rmsnorm(readout, head_gain).astype(BF).reshape(seq_rows, head_dim)
    heads = jnp.broadcast_to(head_out[None], (cores, seq_rows, head_dim))
    heads, parts = lax.optimization_barrier((heads, parts))
    heads = exchanged(heads, ("ep_1", "ep_2"))
    terms = vmem_call(
        project_body, jax.ShapeDtypeStruct((cores, n_tp, seq_rows, 128), BF), (heads, parts)
    )
    terms = exchanged(
        terms.reshape(cores * n_tp, seq_rows, 128), ("ep_1", "ep_2", "tp")
    ).reshape(terms.shape)
    token_slice = lax.dynamic_slice_in_dim(tokens, here * slice_width, slice_width, 1)
    resid, send = vmem_call(
        functools.partial(dispatch_body, piece=piece),
        (
            jax.ShapeDtypeStruct((seq_rows, slice_width), BF),
            jax.ShapeDtypeStruct((slots_all, slice_width), BF),
        ),
        (terms, token_slice, chosen),
    )
    arrived = exchanged(send.reshape(n_z, 2 * cores, slice_width), "ep_0")
    mine = jnp.stack([turned(resid, k, n_tp) for k in range(n_tp)])
    spread = vmem_call(
        spread_body,
        jax.ShapeDtypeStruct((cores, n_tp, 2 * n_z, slice_width), BF),
        (arrived.reshape(slots_all, slice_width),),
    )
    plane = (cores * n_tp, 2 * n_z, slice_width)
    x = exchanged(spread.reshape(plane), ("ep_1", "ep_2", "tp")).reshape(spread.shape)
    down_terms = expert_kernel(x, gain_ffn[None], expert_gate[0], expert_up[0], expert_down[0])
    down_terms = exchanged(down_terms.reshape(plane), ("ep_1", "ep_2", "tp"))
    shared = lax.all_gather(parts[:, 1:], "ep_1")
    other = lax.ppermute(shared, "ep_2", [(0, 1), (1, 0)])
    first = lax.axis_index("ep_2") == 0
    shared = jnp.stack([jnp.where(first, shared, other), jnp.where(first, other, shared)])
    shared = shared.transpose(3, 2, 1, 0, 4, 5).reshape(3, model_width, head_dim)
    shared_terms, mix = shared_kernel(
        here.astype(jnp.int32)[None],
        mine,
        gain_ffn.reshape(n_tp, slice_width).astype(F32),
        w_branch_gate.reshape(n_tp, slice_width).astype(F32),
        shared[0],
        shared[1],
        shared[2],
    )
    shared_parts = [turned(shared_terms[k], k, n_tp) for k in range(n_tp)]
    summed, shared_out = vmem_call(
        collect_body,
        (
            jax.ShapeDtypeStruct((slots_all, slice_width), BF),
            jax.ShapeDtypeStruct((seq_rows, slice_width), BF),
        ),
        (down_terms.reshape(spread.shape), *shared_parts),
    )
    returned = exchanged(summed.reshape(n_z, 2 * cores, slice_width), "ep_0")
    returned = returned.reshape(slots_all, slice_width)
    branch_sum, squares = vmem_call(
        combine_body,
        (
            jax.ShapeDtypeStruct((seq_rows, slice_width), F32),
            jax.ShapeDtypeStruct((n_tp, 8, 128), F32),
        ),
        (combine, returned, shared_out, mix),
    )
    layer_out = vmem_call(
        final_body,
        jax.ShapeDtypeStruct((seq_rows, slice_width), BF),
        (exchanged(squares, "tp"), branch_sum, resid, gain_post.astype(F32)[None]),
    )
    return (layer_out, new_state)


def solution(mesh):
    torus = Mesh(mesh.devices.reshape(16, 4, 2, mesh.shape["tp"]), ("ep_0", "ep_1", "ep_2", "tp"))
    in_specs = (
        P(EP, None),
        P(EP, "tp", None, None),
        P(None, "tp"),
        P(None, "tp"),
        P(None, "tp"),
        P("tp", None),
        P("tp", None),
        P("tp", EP),
        P(),
        P(),
        P("tp"),
        P(),
        P(EP, "tp"),
        P(EP, "tp"),
        P("tp", EP),
        P(EP, None),
        P(EP, None),
        P(EP, None, "tp"),
        P(EP, None, "tp"),
        P(EP, "tp", None),
    )
    out_specs = (P(EP, "tp"), P(EP, "tp", None, None))

    return jax.shard_map(
        shards, mesh=torus, in_specs=in_specs, out_specs=out_specs, check_vma=False
    )
```

```python
import functools

import jax
import jax.numpy as jnp
from jax import lax
from jax.experimental import pallas as pl
from jax.experimental.pallas import tpu as pltpu
from jax.sharding import Mesh
from jax.sharding import PartitionSpec as P

EP = ("ep_0", "ep_1", "ep_2")
epsilon = 1e-06
BF = jnp.bfloat16
F32 = jnp.float32
NT = (((1,), (1,)), ((), ()))


def exchanged(value, axes):
    return lax.all_to_all(value, axes, 0, 0, tiled=True)


def to_all(value, axes):
    devices = lax.axis_size(axes)
    return exchanged(jnp.broadcast_to(value[None], (devices, *value.shape)), axes)


def turned(value, step, devices):
    if step == 0:
        return value
    return lax.ppermute(value, "tp", [(k, (k + step) % devices) for k in range(devices)])


def rmsnorm(values_in, gain):
    scale = lax.rsqrt(jnp.mean(values_in * values_in, axis=-1, keepdims=True) + epsilon)
    return values_in * scale * gain.astype(F32)


def from_z_order(cores, zs, inverse):
    n = cores * zs * 2
    core_major = lax.broadcasted_iota(jnp.int32, (n, n), 1 if inverse else 0)
    z_major = lax.broadcasted_iota(jnp.int32, (n, n), 0 if inverse else 1)
    core = core_major >> (2 * zs).bit_length() - 1
    z = (core_major >> 1) & (zs - 1)
    place = (((z << cores.bit_length() - 1) | core) << 1) | (core_major & 1)
    return jnp.where(z_major == place, 1.0, 0.0).astype(BF)


def vmem_call(body, out_shape, args, scratch=(), limit=32):
    vmem = pl.BlockSpec(memory_space=pltpu.VMEM)
    return pl.pallas_call(
        body,
        out_shape=out_shape,
        in_specs=[vmem] * len(args),
        out_specs=jax.tree.map(lambda _: vmem, out_shape),
        scratch_shapes=list(scratch),
        compiler_params=pltpu.CompilerParams(vmem_limit_bytes=limit * 1024 * 1024),
    )(*args)


def project_body(heads, parts, out):
    cores, n_tp, rows, lanes = out.shape
    n_z = parts.shape[0]
    near = n_z // n_tp
    acts = heads[...].reshape(cores * rows, heads.shape[2])
    for t in range(n_tp):
        start = t * near
        other = (t ^ 1) * near
        order = list(range(start, start + near)) + list(range(other, other + near))
        columns = jnp.concatenate([parts[z, 0] for z in order], axis=0)
        term = lax.dot_general(acts, columns, NT, preferred_element_type=F32).astype(BF)
        out[:, t] = term.reshape(cores, rows, lanes)


def dispatch_body(terms, tok, chosen, resid, send, *, piece):
    cores, n_tp, rows, lanes = terms.shape
    parts = []
    for k in range(cores):
        part = terms[k, 0].astype(F32)
        for t in range(1, n_tp):
            part = part + terms[k, t].astype(F32)
        parts.append(part.astype(BF).astype(F32))
    owner = lax.broadcasted_iota(jnp.int32, (rows, lanes), 1) // piece
    for z in range(tok.shape[1] // lanes):
        mixed = jnp.zeros((rows, lanes), F32)
        for k in range(cores):
            turn = (k - z) * piece % lanes
            moved = pltpu.roll(parts[k], turn, 1) if turn else parts[k]
            mixed = jnp.where(owner == k, moved, mixed)
        cols = pl.ds(z * lanes, lanes)
        resid[:, cols] = (tok[:, cols].astype(F32) + mixed).astype(BF)
    send[...] = jnp.dot(chosen[...], resid[...], preferred_element_type=F32).astype(BF)


def spread_body(arrived, out):
    cores, n_tp, rows, width = out.shape
    perm = from_z_order(cores, rows // 2, False)
    moved = jnp.dot(perm, arrived[...], preferred_element_type=F32).astype(BF)
    for t in range(n_tp):
        out[:, t] = moved.reshape(cores, rows, width)


def combine_body(weights, returned, shared, mix, branch, squares):
    rest = weights[...]
    total = mix[:, :1] * shared[...].astype(F32)
    for _ in range(3):
        part = rest.astype(BF)
        rest = rest - part.astype(F32)
        total = total + jnp.dot(part, returned[...], preferred_element_type=F32)
    branch[...] = total
    square = jnp.sum(total * total, axis=1, keepdims=True)
    group = lax.broadcasted_iota(jnp.int32, squares.shape[1:], 1)
    packed = jnp.zeros(squares.shape[1:], F32)
    for g in range(total.shape[0] // 8):
        packed = jnp.where(group == g, square[8 * g : 8 * g + 8], packed)
    squares[...] = jnp.broadcast_to(packed[None], squares.shape)


def final_body(squares, branch, resid, gain, out):
    n_tp = squares.shape[0]
    total = squares[0]
    for t in range(1, n_tp):
        total = total + squares[t]
    scale = lax.rsqrt(total / (n_tp * out.shape[1]) + epsilon)
    for g in range(out.shape[0] // 8):
        rows = pl.ds(8 * g, 8)
        grown = branch[rows, :] * scale[:, g : g + 1] * gain[...]
        out[rows, :] = (resid[rows, :].astype(F32) + grown).astype(BF)


def collect_body(terms, first, second, third, fourth, out, shared):
    parts = [r[...].astype(F32) for r in (first, second, third, fourth)]
    shared[...] = (parts[0] + parts[1] + parts[2] + parts[3]).astype(BF)
    cores, n_tp, rows, width = terms.shape
    total = terms[:, 0].astype(F32)
    for t in range(1, n_tp):
        total = total + terms[:, t].astype(F32)
    perm = from_z_order(cores, rows // 2, True)
    total = total.astype(BF).reshape(cores * rows, width)
    out[...] = jnp.dot(perm, total, preferred_element_type=F32).astype(BF)


def normed_columns(x, gain, hn):
    slice_width = hn.shape[1] // x[0]
    squares = None
    for j in range(x[0]):
        wide = x[1](j).astype(F32)
        part = jnp.sum(wide * wide, axis=1, keepdims=True)
        squares = part if squares is None else squares + part
    scale = lax.rsqrt(squares / hn.shape[1] + epsilon)
    for j in range(x[0]):
        cols = pl.ds(j * slice_width, slice_width)
        hn[:, cols] = (x[1](j).astype(F32) * scale * gain[:, cols].astype(F32)).astype(BF)


def expert_body(
    x, gain, gate_hbm, up_hbm, down_hbm, out, hn, gate_w, up_w, down_w, held, sems, sent
):
    cores, n_tp, rows, slice_width = x.shape
    total = cores * rows
    copies = [
        pltpu.make_async_copy(src, dst, sems.at[k])
        for k, (src, dst) in enumerate(
            ((gate_hbm, gate_w), (up_hbm, up_w), (down_hbm, down_w))
        )
    ]
    for copy in copies:
        copy.start()
    normed_columns((n_tp, lambda j: x[:, j].reshape(total, slice_width)), gain, hn)
    copies[0].wait()
    gate_pre = jnp.dot(hn[...], gate_w[...], preferred_element_type=F32)
    copies[1].wait()
    up_pre = jnp.dot(hn[...], up_w[...], preferred_element_type=F32)
    hidden = (gate_pre * jax.nn.sigmoid(gate_pre) * up_pre).astype(BF)
    copies[2].wait()
    for j in range(n_tp):
        cols = pl.ds(j * slice_width, slice_width)
        part = jnp.dot(hidden, down_w[:, cols], preferred_element_type=F32).astype(BF)
        held[j] = part.reshape(cores, rows, slice_width)
        copies.append(pltpu.make_async_copy(held.at[j], out.at[:, j], sent.at[j]))
        copies[-1].start()
    for copy in copies[3:]:
        copy.wait()


def expert_kernel(x, gain, gate_w, up_w, down_w):
    cores, n_tp, rows, slice_width = x.shape
    vmem = pl.BlockSpec(memory_space=pltpu.VMEM)
    hbm = pl.BlockSpec(memory_space=pl.ANY)
    return pl.pallas_call(
        expert_body,
        out_shape=jax.ShapeDtypeStruct(x.shape, BF),
        in_specs=[vmem, vmem, hbm, hbm, hbm],
        out_specs=hbm,
        scratch_shapes=[
            pltpu.VMEM((cores * rows, n_tp * slice_width), BF),
            pltpu.VMEM(gate_w.shape, BF),
            pltpu.VMEM(up_w.shape, BF),
            pltpu.VMEM(down_w.shape, BF),
            pltpu.VMEM((n_tp, cores, rows, slice_width), BF),
            pltpu.SemaphoreType.DMA((3,)),
            pltpu.SemaphoreType.DMA((n_tp,)),
        ],
        compiler_params=pltpu.CompilerParams(vmem_limit_bytes=32 * 1024 * 1024),
        name="expert",
    )(x, gain, gate_w, up_w, down_w)


def shared_body(place, x, gain, mix_w, gate_w, up_w, down_w, out, mix):
    n_tp, rows, slice_width = x.shape
    here = place[0]
    squares = jnp.zeros((rows, 1), F32)
    for k in range(n_tp):
        wide = x[k].astype(F32)
        squares = squares + jnp.sum(wide * wide, axis=1, keepdims=True)
    scale = lax.rsqrt(squares / (n_tp * slice_width) + epsilon)
    logits = jnp.zeros((rows, 1), F32)
    gate_pre = jnp.zeros((rows, gate_w.shape[1]), F32)
    up_pre = jnp.zeros((rows, up_w.shape[1]), F32)
    for k in range(n_tp):
        j = lax.rem(here + (n_tp - k), n_tp)
        cols = pl.ds(pl.multiple_of(j * slice_width, slice_width), slice_width)
        part = (x[k].astype(F32) * scale * gain[pl.ds(j, 1), :].astype(F32)).astype(BF)
        logits = logits + jnp.sum(
            part.astype(F32) * mix_w[pl.ds(j, 1), :].astype(F32), axis=1, keepdims=True
        )
        gate_pre = gate_pre + jnp.dot(part, gate_w[cols, :], preferred_element_type=F32)
        up_pre = up_pre + jnp.dot(part, up_w[cols, :], preferred_element_type=F32)
    mix[...] = jnp.broadcast_to(jax.nn.sigmoid(logits), mix.shape)
    hidden = (gate_pre * jax.nn.sigmoid(gate_pre) * up_pre).astype(BF)
    for k in range(n_tp):
        j = lax.rem(here + k, n_tp)
        cols = pl.ds(pl.multiple_of(j * slice_width, slice_width), slice_width)
        out[k] = lax.dot_general(hidden, down_w[cols, :], NT, preferred_element_type=F32).astype(BF)


def shared_kernel(place, *args):
    n_tp, rows, slice_width = args[0].shape
    vmem = pl.BlockSpec(memory_space=pltpu.VMEM)
    smem = pl.BlockSpec(memory_space=pltpu.SMEM)
    return pl.pallas_call(
        shared_body,
        out_shape=(
            jax.ShapeDtypeStruct((n_tp, rows, slice_width), BF),
            jax.ShapeDtypeStruct((rows, 128), F32),
        ),
        in_specs=[smem] + [vmem] * len(args),
        out_specs=(vmem, vmem),
        compiler_params=pltpu.CompilerParams(vmem_limit_bytes=16 * 1024 * 1024),
        name="shared",
    )(place, *args)


def shards(
    tokens,
    carried_state,
    w_query,
    w_forget,
    w_value,
    forget_floor,
    head_gain,
    w_out,
    gain_mix,
    gain_ffn,
    gain_post,
    w_branch_gate,
    shared_gate,
    shared_up,
    shared_down,
    routes,
    route_weights,
    expert_gate,
    expert_up,
    expert_down,
):
    seq_rows, model_width = tokens.shape
    head_dim = carried_state.shape[2]
    n_ep = lax.axis_size(EP)
    n_z = lax.axis_size("ep_0")
    n_tp = lax.axis_size("tp")
    cores = n_ep // n_z
    piece = w_out.shape[1]
    slice_width = model_width // n_tp
    slots_all = 2 * n_ep
    here = lax.axis_index("tp")
    parts = to_all(jnp.stack([w_out.T, shared_gate, shared_up, shared_down.T]), "ep_0")
    column = lax.broadcasted_iota(jnp.int32, (1, 1, slots_all), 2)
    hits = routes[:, :, None] == column // 2
    named = jnp.any(hits, axis=1).astype(BF)
    tri = (
        lax.broadcasted_iota(jnp.int32, (seq_rows, seq_rows), 0)
        > lax.broadcasted_iota(jnp.int32, (seq_rows, seq_rows), 1)
    ).astype(BF)
    rank = jnp.dot(tri, named, preferred_element_type=F32)
    taken = (named > 0) & (rank == (column[0] % 2).astype(F32))
    chosen = jnp.where(taken, 1.0, 0.0).astype(BF).T
    combine = jnp.where(hits, route_weights[:, :, None], 0.0)
    combine = jnp.where(taken, jnp.sum(combine, axis=1), 0.0)
    normed = rmsnorm(tokens.astype(F32), gain_mix).astype(BF)
    queries = jax.nn.silu(jnp.dot(normed, w_query, preferred_element_type=F32))
    forget_pre = jnp.dot(normed, w_forget, preferred_element_type=F32)
    values_in = jnp.dot(normed, w_value, preferred_element_type=F32)
    queries = queries.reshape(seq_rows, 1, head_dim)
    forget_pre = forget_pre.reshape(seq_rows, 1, head_dim)
    values_in = values_in.reshape(seq_rows, 1, head_dim)
    forget = forget_floor + (1.0 - forget_floor) * jax.nn.sigmoid(forget_pre)
    keys_in = (1.0 - forget_floor) * jax.nn.sigmoid(-forget_pre)
    new_state = forget[..., None] * carried_state + keys_in[..., None] * values_in[:, :, None, :]
    readout = jnp.einsum("bhd,bhdv->bhv", queries, new_state, precision=lax.Precision.HIGHEST)
    head_out = rmsnorm(readout, head_gain).astype(BF).reshape(seq_rows, head_dim)
    heads = jnp.broadcast_to(head_out[None], (cores, seq_rows, head_dim))
    heads, parts = lax.optimization_barrier((heads, parts))
    heads = exchanged(heads, ("ep_1", "ep_2"))
    terms = vmem_call(
        project_body, jax.ShapeDtypeStruct((cores, n_tp, seq_rows, 128), BF), (heads, parts)
    )
    terms = exchanged(
        terms.reshape(cores * n_tp, seq_rows, 128), ("ep_1", "ep_2", "tp")
    ).reshape(terms.shape)
    token_slice = lax.dynamic_slice_in_dim(tokens, here * slice_width, slice_width, 1)
    resid, send = vmem_call(
        functools.partial(dispatch_body, piece=piece),
        (
            jax.ShapeDtypeStruct((seq_rows, slice_width), BF),
            jax.ShapeDtypeStruct((slots_all, slice_width), BF),
        ),
        (terms, token_slice, chosen),
    )
    arrived = exchanged(send.reshape(n_z, 2 * cores, slice_width), "ep_0")
    mine = jnp.stack([turned(resid, k, n_tp) for k in range(n_tp)])
    spread = vmem_call(
        spread_body,
        jax.ShapeDtypeStruct((cores, n_tp, 2 * n_z, slice_width), BF),
        (arrived.reshape(slots_all, slice_width),),
    )
    plane = (cores * n_tp, 2 * n_z, slice_width)
    x = exchanged(spread.reshape(plane), ("ep_1", "ep_2", "tp")).reshape(spread.shape)
    down_terms = expert_kernel(x, gain_ffn[None], expert_gate[0], expert_up[0], expert_down[0])
    down_terms = exchanged(down_terms.reshape(plane), ("ep_1", "ep_2", "tp"))
    shared = lax.all_gather(parts[:, 1:], "ep_1")
    other = lax.ppermute(shared, "ep_2", [(0, 1), (1, 0)])
    first = lax.axis_index("ep_2") == 0
    shared = jnp.stack([jnp.where(first, shared, other), jnp.where(first, other, shared)])
    shared = shared.transpose(3, 2, 1, 0, 4, 5).reshape(3, model_width, head_dim)
    shared_terms, mix = shared_kernel(
        here.astype(jnp.int32)[None],
        mine,
        gain_ffn.reshape(n_tp, slice_width).astype(F32),
        w_branch_gate.reshape(n_tp, slice_width).astype(F32),
        shared[0],
        shared[1],
        shared[2],
    )
    shared_parts = [turned(shared_terms[k], k, n_tp) for k in range(n_tp)]
    summed, shared_out = vmem_call(
        collect_body,
        (
            jax.ShapeDtypeStruct((slots_all, slice_width), BF),
            jax.ShapeDtypeStruct((seq_rows, slice_width), BF),
        ),
        (down_terms.reshape(spread.shape), *shared_parts),
    )
    returned = exchanged(summed.reshape(n_z, 2 * cores, slice_width), "ep_0")
    returned = returned.reshape(slots_all, slice_width)
    branch_sum, squares = vmem_call(
        combine_body,
        (
            jax.ShapeDtypeStruct((seq_rows, slice_width), F32),
            jax.ShapeDtypeStruct((n_tp, 8, 128), F32),
        ),
        (combine, returned, shared_out, mix),
    )
    layer_out = vmem_call(
        final_body,
        jax.ShapeDtypeStruct((seq_rows, slice_width), BF),
        (exchanged(squares, "tp"), branch_sum, resid, gain_post.astype(F32)[None]),
    )
    return (layer_out, new_state)


def solution(mesh):
    torus = Mesh(mesh.devices.reshape(16, 4, 2, mesh.shape["tp"]), ("ep_0", "ep_1", "ep_2", "tp"))
    in_specs = (
        P(EP, None),
        P(EP, "tp", None, None),
        P(None, "tp"),
        P(None, "tp"),
        P(None, "tp"),
        P("tp", None),
        P("tp", None),
        P("tp", EP),
        P(),
        P(),
        P("tp"),
        P(),
        P(EP, "tp"),
        P(EP, "tp"),
        P("tp", EP),
        P(EP, None),
        P(EP, None),
        P(EP, None, "tp"),
        P(EP, None, "tp"),
        P(EP, "tp", None),
    )
    out_specs = (P(EP, "tp"), P(EP, "tp", None, None))

    return jax.shard_map(
        shards, mesh=torus, in_specs=in_specs, out_specs=out_specs, check_vma=False
    )
```
